128 devices in a mesh: sp: 16 (over z, y), tp: 8 (over x, core).
Axes of the slice: x: 4, y: 4, z: 4, core: 2. Of those that a mesh axis runs over, the one named last changes fastest.
Arguments:
- resid: bfloat16 [12288, 2048], P(('sp', 'tp')), may hold values from -6 to 6
- query_small: bfloat16 [12288, 768], P('sp', 'tp'), may hold values from -480 to 480
- query_large: bfloat16 [12288, 1280], P('sp', 'tp'), may hold values from -480 to 480
- kv_latent: bfloat16 [12288, 256], P('sp'), may hold values from -6 to 6
- rope_key: bfloat16 [12288, 32], P('sp'), may hold values from -6 to 6
- kv_gain: bfloat16 [256], replicated, may hold values from 0.099609375 to 1.8984375
- up_key_small: bfloat16 [256, 512], P(None, 'tp'), may hold values from -0.375 to 0.375
- up_value_small: bfloat16 [256, 512], P(None, 'tp'), may hold values from -0.375 to 0.375
- up_key_large: bfloat16 [256, 1024], P(None, 'tp'), may hold values from -0.375 to 0.375
- up_value_large: bfloat16 [256, 1024], P(None, 'tp'), may hold values from -0.375 to 0.375
- out_weight: bfloat16 [1536, 2048], replicated, may hold values from -0.359375 to 0.359375
- mix_gain: bfloat16 [2048], replicated, may hold values from 0.099609375 to 1.8984375
- gate_weight: bfloat16 [2048, 5632], P('sp', 'tp'), may hold values from -0.125 to 0.125
- up_weight: bfloat16 [2048, 5632], P('sp', 'tp'), may hold values from -0.125 to 0.125
- down_weight: bfloat16 [2048, 5632], P('sp', 'tp'), may hold values from -0.078125 to 0.078125
Outputs:
- layer_output: bfloat16 [12288, 2048], P(('sp', 'tp'))
The draws below stay inside these ranges and needn't reach their ends.
All inputs are finite; a program needn't handle non-finite values.
Results may differ from the reference program's by a relative error of at most 0.014.
The reference program's roundings to bfloat16 on the way count: a program that leaves them out, or rounds other values in their place, can miss the bound.
Values may be sent and summed in bfloat16 or wider, within the bound.
A program may use at most 128 MiB of HBM per device.

```python
import math
import jax
import jax.numpy as jnp
from jax import lax

D = 2048
HEADS_SMALL = 8
HEADS_LARGE = 8
NOPE_SMALL = 64
NOPE_LARGE = 128
VALUE_SMALL = 64
VALUE_LARGE = 128
ROTARY = 32
LATENT = 256
FF = 5632
TOK_DEV = 768
SEQ = 12288
N_TP = 8


def drawn_query(key, columns):
    base = 2.0 * jax.random.truncated_normal(key, -6.0, 6.0, (SEQ, columns), jnp.float32)
    return base


def draw_query_small(key, part):
    return drawn_query(jax.random.fold_in(key, 11), HEADS_SMALL * (NOPE_SMALL + ROTARY)).astype(jnp.bfloat16)


def draw_query_large(key, part):
    return drawn_query(jax.random.fold_in(key, 13), HEADS_LARGE * (NOPE_LARGE + ROTARY)).astype(jnp.bfloat16)


def steps_of(key, shape, split, low, high):
    loudness = 1.0
    for dim, shards_of in split:
        steps = jax.random.uniform(jax.random.fold_in(jax.random.fold_in(key, 6), dim), (shards_of,), jnp.float32, low / len(split), high / len(split))
        loudness = loudness * jnp.repeat(jnp.exp(steps), shape[dim] // shards_of).reshape((-1,) + (1,) * (len(shape) - 1 - dim))
    return loudness


def normal_values(own_key, extent, scale, bound, shards=(), held_as=jnp.bfloat16):
    factor_of = steps_of(own_key, extent, shards, -0.22, 0.18) if shards else 1.0
    drawn = jax.random.normal(own_key, extent, jnp.float32) * scale * factor_of
    return jnp.minimum(jnp.maximum(drawn, -bound), bound).astype(held_as)


def setup_inputs(seed: int = 0) -> dict:
    arg_keys = jax.random.split(jax.random.key(seed), 16)
    return {
        "resid": normal_values(arg_keys[0], (SEQ, D), 1.0, 6.0, ((0, 128),)),
        "query_small": draw_query_small(jax.random.fold_in(arg_keys[15], 71), 0),
        "query_large": draw_query_large(jax.random.fold_in(arg_keys[15], 71), 0),
        "kv_latent": normal_values(arg_keys[3], (SEQ, LATENT), 1.0, 6.0, ((0, 16),)),
        "rope_key": normal_values(arg_keys[4], (SEQ, ROTARY), 1.0, 6.0, ((0, 16),)),
        "kv_gain": jnp.clip(1.0 + 0.18 * jax.random.normal(arg_keys[5], (LATENT,), jnp.float32), 0.099609375, 1.8984375).astype(jnp.bfloat16),
        "up_key_small": normal_values(arg_keys[6], (LATENT, HEADS_SMALL * NOPE_SMALL), LATENT ** -0.5, 0.375, ((1, 8),)),
        "up_value_small": normal_values(arg_keys[7], (LATENT, HEADS_SMALL * VALUE_SMALL), LATENT ** -0.5, 0.375, ((1, 8),)),
        "up_key_large": normal_values(arg_keys[8], (LATENT, HEADS_LARGE * NOPE_LARGE), LATENT ** -0.5, 0.375, ((1, 8),)),
        "up_value_large": normal_values(arg_keys[9], (LATENT, HEADS_LARGE * VALUE_LARGE), LATENT ** -0.5, 0.375, ((1, 8),)),
        "out_weight": normal_values(arg_keys[10], (HEADS_SMALL * VALUE_SMALL + HEADS_LARGE * VALUE_LARGE, D), 0.06, 0.359375),
        "mix_gain": jnp.clip(1.0 + 0.18 * jax.random.normal(arg_keys[11], (D,), jnp.float32), 0.099609375, 1.8984375).astype(jnp.bfloat16),
        "gate_weight": normal_values(arg_keys[12], (D, FF), D ** -0.5, 0.125, ((0, 16), (1, 8))),
        "up_weight": normal_values(arg_keys[13], (D, FF), D ** -0.5, 0.125, ((0, 16), (1, 8))),
        "down_weight": normal_values(arg_keys[14], (D, FF), FF ** -0.5, 0.078125, ((0, 16), (1, 8))),
    }


THETA = 10000.0
EPSILON = 1e-06
FLOOR = -1e+30

def angles(positions, width):
    inverse = THETA ** (-jnp.arange(0, width, 2).astype(jnp.float32) / width)
    phase = positions.astype(jnp.float32)[:, None] * inverse[None, :]
    return (jnp.cos(phase), jnp.sin(phase))

def rotate(values, angle_cos, angle_sin):
    half = values.shape[-1] // 2
    first = values[..., :half].astype(jnp.float32)
    second = values[..., half:].astype(jnp.float32)
    turned = jnp.concatenate([first * angle_cos - second * angle_sin, second * angle_cos + first * angle_sin], axis=-1)
    return turned.astype(jnp.bfloat16)

def norm_rows(values, gain):
    wide = values.astype(jnp.float32)
    scaled = wide * lax.rsqrt(lax.optimization_barrier(jnp.mean(wide * wide, axis=-1, keepdims=True)) + EPSILON)
    return (scaled * gain.astype(jnp.float32)).astype(jnp.bfloat16)

def attend(query, key_nope, shared_key, values, nope):
    length = query.shape[0]
    heads = query.shape[1]
    scale = 1.0 / math.sqrt(nope + shared_key.shape[1])
    count = length // TOK_DEV
    key_wide = key_nope.astype(jnp.float32)
    shared_wide = shared_key.astype(jnp.float32)
    value_wide = values.astype(jnp.float32)

    def one_block(index):
        start = index * TOK_DEV
        block = lax.dynamic_slice_in_dim(query, start, TOK_DEV, 0).astype(jnp.float32)
        scores = jnp.einsum('qhd,khd->hqk', block[..., :nope], key_wide)
        scores = scores + jnp.einsum('qhd,kd->hqk', block[..., nope:], shared_wide)
        scores = scores * scale
        query_pos = start + jnp.arange(TOK_DEV).astype(jnp.int32)
        key_pos = jnp.arange(length).astype(jnp.int32)
        allowed = key_pos[None, :] <= query_pos[:, None]
        scores = jnp.where(allowed[None], scores, FLOOR)
        maximum = lax.optimization_barrier(jnp.max(scores, axis=-1, keepdims=True))
        weights = jnp.where(allowed[None], jnp.exp(scores - maximum), 0.0)
        total = lax.optimization_barrier(jnp.sum(weights, axis=-1))
        rounded = lax.optimization_barrier(weights.astype(jnp.bfloat16)).astype(jnp.float32)
        summed = jnp.einsum('hqk,khd->qhd', rounded, value_wide)
        return (summed / jnp.transpose(total)[:, :, None]).astype(jnp.bfloat16)
    out = lax.map(one_block, jnp.arange(count).astype(jnp.int32))
    return out.reshape(length, -1)

def reference(resid, query_small, query_large, kv_latent, rope_key, kv_gain, up_key_small, up_value_small, up_key_large, up_value_large, out_weight, mix_gain, gate_weight, up_weight, down_weight):
    length = kv_latent.shape[0]
    positions = jnp.arange(length).astype(jnp.int32)
    angle_cos, angle_sin = angles(positions, ROTARY)
    latent_normed = norm_rows(kv_latent, kv_gain)
    rotated_key = rotate(rope_key, angle_cos, angle_sin)

    def group(query, up_key, up_value, heads, nope, width):
        shaped = query.reshape(length, heads, nope + ROTARY)
        turned = rotate(shaped[..., nope:], angle_cos[:, None, :], angle_sin[:, None, :])
        full_query = jnp.concatenate([shaped[..., :nope], turned], axis=-1)
        keys = jnp.dot(latent_normed, up_key, preferred_element_type=jnp.float32).astype(jnp.bfloat16)
        values = jnp.dot(latent_normed, up_value, preferred_element_type=jnp.float32).astype(jnp.bfloat16)
        return attend(full_query, keys.reshape(length, heads, nope), rotated_key, values.reshape(length, heads, width), nope)
    attn_small = group(query_small, up_key_small, up_value_small, HEADS_SMALL, NOPE_SMALL, VALUE_SMALL)
    attn_large = group(query_large, up_key_large, up_value_large, HEADS_LARGE, NOPE_LARGE, VALUE_LARGE)
    border = HEADS_SMALL * VALUE_SMALL
    mixed = jnp.dot(attn_small, out_weight[:border], preferred_element_type=jnp.float32)
    mixed = mixed + jnp.dot(attn_large, out_weight[border:], preferred_element_type=jnp.float32)
    middle = (resid.astype(jnp.float32) + mixed).astype(jnp.bfloat16)
    middle_wide = lax.optimization_barrier(middle).astype(jnp.float32)
    mixer_in = norm_rows(middle, mix_gain)
    gate = jnp.dot(mixer_in, gate_weight, preferred_element_type=jnp.float32)
    upward = jnp.dot(mixer_in, up_weight, preferred_element_type=jnp.float32)
    hidden = (jax.nn.silu(gate) * upward).astype(jnp.bfloat16)
    width = FF // N_TP
    total = middle_wide
    for index in range(N_TP):
        part = jnp.dot(hidden[:, index * width:(index + 1) * width], jnp.transpose(down_weight[:, index * width:(index + 1) * width]), preferred_element_type=jnp.float32).astype(jnp.bfloat16)
        total = total + lax.optimization_barrier(part).astype(jnp.float32)
    return total.astype(jnp.bfloat16)
```

```python
import functools
import math

import jax
import jax.numpy as jnp
from jax import lax
from jax.experimental import pallas as pl
from jax.experimental.pallas import tpu as pltpu
from jax.sharding import PartitionSpec as P

NOPE_SMALL = 64
NOPE_LARGE = 128
ROTARY = 32
THETA = 10000.0
EPSILON = 1e-06
FLOOR = -1e30
ROWS = 768
LAT_ROWS = 896
D = 2048
OWN = 96
FFD = 704
QT = 256
MT = 256
F32 = jnp.float32
BF16 = jnp.bfloat16


def angles(positions, width):
    inverse = THETA ** (-jnp.arange(0, width, 2).astype(F32) / width)
    phase = positions.astype(F32)[:, None] * inverse[None, :]
    return (jnp.cos(phase), jnp.sin(phase))


def rotate(values, angle_cos, angle_sin):
    half = values.shape[-1] // 2
    first = values[..., :half].astype(F32)
    second = values[..., half:].astype(F32)
    turned = jnp.concatenate(
        [first * angle_cos - second * angle_sin, second * angle_cos + first * angle_sin], axis=-1
    )
    return turned.astype(BF16)


def norm_rows(values, gain):
    wide = values.astype(F32)
    scaled = wide * lax.rsqrt(jnp.mean(wide * wide, axis=-1, keepdims=True) + EPSILON)
    return (scaled * gain.astype(F32)).astype(BF16)


def dot(a, b, ca=1, cb=0):
    return lax.dot_general(a, b, (((ca,), (cb,)), ((), ())), preferred_element_type=F32)


class Flow:
    def __init__(self, view, size, send_sem, recv_sem, block, target):
        self.view, self.size = view, size
        self.send_sem, self.recv_sem = send_sem, recv_sem
        self.block, self.target = block, target
        self.sent = []

    def copy(self, at, lo, size, to, k):
        ref = self.view(self.block(*at), lo, size)
        return pltpu.make_async_remote_copy(
            src_ref=ref,
            dst_ref=ref,
            send_sem=self.send_sem.at[k],
            recv_sem=self.recv_sem.at[k],
            device_id=self.target(*to),
            device_id_type=pl.DeviceIdType.MESH,
        )

    def send(self, at, part, to, k):
        lo, size = self.span(part)
        self.sent.append((at, lo, size, to, k))
        self.copy(at, lo, size, to, k).start()

    def span(self, part):
        half = self.size // 2
        return {None: (0, self.size), 0: (0, half), 1: (half, half)}[part]

    def wait(self, at, part, k):
        lo, size = self.span(part)
        self.copy(at, lo, size, (1, 0), k).wait_recv()

    def finish(self):
        for at, lo, size, to, k in self.sent:
            self.copy(at, lo, size, to, k).wait_send()

    def start_u(self):
        self.send((0, 0), None, (1, 0), 0)
        self.send((0, 0), None, (-1, 0), 1)

    def spread(self, du, k):
        self.send((du, 0), None, (0, 1), k)
        self.send((du, 0), None, (0, -1), k + 1)

    def relay_v(self, du, k):
        self.wait((du, -1), None, k)
        self.send((du, -1), 0, (0, 1), k + 2)
        self.wait((du, 1), None, k + 1)
        self.send((du, 1), 1, (0, -1), k + 3)

    def end_v(self, du, k):
        self.wait((du, 2), 0, k + 2)
        self.wait((du, 2), 1, k + 3)

    def event(self, n):
        if n == 0:
            self.start_u()
            self.spread(0, 4)
        elif n == 1:
            self.wait((-1, 0), None, 0)
            self.send((-1, 0), 0, (1, 0), 2)
            self.spread(-1, 8)
        elif n == 2:
            self.wait((1, 0), None, 1)
            self.send((1, 0), 1, (-1, 0), 3)
            self.spread(1, 12)
        elif n == 3:
            self.relay_v(0, 4)
        elif n == 4:
            self.wait((2, 0), 0, 2)
            self.wait((2, 0), 1, 3)
            self.spread(2, 16)
        elif n == 5:
            self.relay_v(-1, 8)
        elif n == 6:
            self.relay_v(1, 12)
        elif n == 7:
            self.relay_v(2, 16)
        else:
            du = (0, -1, 1, 2)[n - 8]
            self.end_v(du, 4 + 4 * (n - 8))

    def line(self, n):
        if n == 0:
            self.start_u()
        elif n == 1:
            self.wait((-1, 0), None, 0)
            self.send((-1, 0), 0, (1, 0), 2)
        elif n == 2:
            self.wait((1, 0), None, 1)
            self.send((1, 0), 1, (-1, 0), 3)
        elif n == 3:
            self.wait((2, 0), 0, 2)
            self.wait((2, 0), 1, 3)


def done_at(du, dv):
    if dv == 0:
        return {0: 0, -1: 1, 1: 2, 2: 4}[du]
    if dv == 2:
        return 8 + (0, -1, 1, 2).index(du)
    return {0: 3, -1: 5, 1: 6, 2: 7}[du]


def kernel(
    lat_hbm, qs_ref, ql_ref, wk_ref, wv_ref, ow_hbm, res_hbm, gain_ref, w_hbm,
    out_ref,
    lbuf, wbuf, owbuf, mid, nbuf, obuf, abuf, ks, kl, vs, vl, ms, ml, acs, acl,
    hbuf, po, xs, xr, ra, rb, fa, fb, st, so,
    cp, la_s, la_r, lb_s, lb_r, wa_s, wa_r, wb_s, wb_r, ls_s, ls_r,
    r_s, r_r, rs_s, rs_r, o_s, o_r, os_s, os_r, d_s, d_r, f_s, f_r,
):
    sp, tp = lax.axis_index("sp"), lax.axis_index("tp")
    z, y = sp // 4, lax.rem(sp, 4)
    x, core = tp // 2, lax.rem(tp, 2)
    mesh_id = pl.DeviceIdType.MESH

    def at_sp(dy, dz):
        return lax.rem(z + dz + 4, 4) * 4 + lax.rem(y + dy + 4, 4)

    def at_x(dx, _=0):
        return lax.rem(x + dx + 4, 4)

    sibling = {"tp": x * 2 + 1 - core}
    near = [{"sp": at_sp(*d)} for d in ((1, 0), (-1, 0), (0, 1), (0, -1))]
    near += [{"tp": at_x(d) * 2 + core} for d in (1, -1)] + [sibling]

    local = [
        pltpu.make_async_copy(lat_hbm, lbuf.at[sp], cp.at[0]),
        pltpu.make_async_copy(res_hbm, mid.at[pl.ds(pl.multiple_of(tp * OWN, 32), OWN)], cp.at[1]),
        pltpu.make_async_copy(w_hbm, wbuf.at[pl.ds(pl.multiple_of(sp * 128, 128), 128)], cp.at[2]),
        pltpu.make_async_copy(ow_hbm, owbuf, cp.at[3]),
    ]
    for c in local:
        c.start()
    barrier = pltpu.get_barrier_semaphore()
    for n in near:
        pl.semaphore_signal(barrier, inc=1, device_id=n, device_id_type=mesh_id)
    pl.semaphore_wait(barrier, len(near))

    q_rows = LAT_ROWS // 4

    def lat_view(piece):
        def view(block, lo, size):
            base = pl.multiple_of((core * 2 + piece) * q_rows, 16)
            return lbuf.at[block, pl.ds(base + lo, size)]
        return view

    def w_view(piece):
        def view(block, lo, size):
            return wbuf.at[pl.ds(pl.multiple_of(block * 128, 128) + 64 * piece + lo, size)]
        return view

    def yz(du, dv):
        return at_sp(du, dv)

    def zy(du, dv):
        return at_sp(dv, du)

    def to_yz(du, dv):
        return {"sp": at_sp(du, dv)}

    def to_zy(du, dv):
        return {"sp": at_sp(dv, du)}

    def to_x(du, _):
        return {"tp": at_x(du) * 2 + core}

    lat_a = Flow(lat_view(0), q_rows, la_s, la_r, yz, to_yz)
    lat_b = Flow(lat_view(1), q_rows, lb_s, lb_r, zy, to_zy)
    w_a = Flow(w_view(0), 64, wa_s, wa_r, yz, to_yz)
    w_b = Flow(w_view(1), 64, wb_s, wb_r, zy, to_zy)

    def res_view(chip, lo, size, c=None):
        c = core if c is None else c
        return mid.at[pl.ds(pl.multiple_of((chip * 2 + c) * OWN, 32) + lo, size)]

    def o_view(chip, lo, size, c=None):
        c = core if c is None else c
        return obuf.at[chip * 2 + c, pl.ds(lo, size)]

    res = Flow(res_view, OWN, r_s, r_r, at_x, to_x)
    att = Flow(o_view, 1152, o_s, o_r, at_x, to_x)

    def beside(src, dst, s, r):
        return pltpu.make_async_remote_copy(
            src_ref=src, dst_ref=dst, send_sem=s, recv_sem=r, device_id=sibling, device_id_type=mesh_id
        )

    def share_lat(rel, c=None):
        base = pl.multiple_of((core if c is None else c) * (2 * q_rows), 64)
        ref = lbuf.at[at_sp(*rel), pl.ds(base, 2 * q_rows)]
        n = (rel[1] % 4) * 4 + rel[0] % 4
        return beside(ref, ref, ls_s.at[n], ls_r.at[n])

    def share_line(view, size, s, r, dx, c=None):
        ref = view(at_x(dx), 0, size, c)
        return beside(ref, ref, s.at[dx % 4], r.at[dx % 4])

    share_res = functools.partial(share_line, res_view, OWN, rs_s, rs_r)
    share_att = functools.partial(share_line, o_view, 1152, os_s, os_r)

    others = [(dy, dz) for dz in (0, 1, -1, 2) for dy in (0, 1, -1, 2) if (dy, dz) != (0, 0)]

    def lat_event(n):
        lat_a.event(n)
        lat_b.event(n)
        for rel in others:
            if max(done_at(*rel), done_at(rel[1], rel[0])) == n:
                share_lat(rel).start()

    scale_small = math.log2(math.e) / math.sqrt(NOPE_SMALL + ROTARY)
    scale_large = math.log2(math.e) / math.sqrt(NOPE_LARGE + ROTARY)

    def expand(block):
        latent = lbuf[block, 0:ROWS, :]
        keys = dot(wk_ref[...], latent, 1, 1).astype(BF16)
        ks[0:64, :] = keys[0:64]
        kl[0:128, :] = keys[64:192]
        for n in range(3):
            turned = lbuf[block, ROWS + 32 * n : ROWS + 32 * n + 32, :]
            ks[64:96, 256 * n : 256 * n + 256] = turned
            kl[128:160, 256 * n : 256 * n + 256] = turned
        values = dot(latent, wv_ref[...]).astype(BF16)
        vl[:, 0:128] = values[:, 0:128]
        vs[:, 0:64] = values[:, 128:192]

    def tile(i, diagonal):
        rows = pl.ds(pl.multiple_of(i * QT, QT), QT)
        for q, k, v, m, acc, scale in (
            (ql_ref, kl, vl, ml, acl, scale_large),
            (qs_ref, ks, vs, ms, acs, scale_small),
        ):
            s = dot(q[rows, :], k[...])
            if diagonal:
                row = lax.broadcasted_iota(jnp.int32, (QT, ROWS), 0) + i * QT
                col = lax.broadcasted_iota(jnp.int32, (QT, ROWS), 1)
                s = jnp.where(col <= row, s, FLOOR)
                new = jnp.max(s, axis=1, keepdims=True)
            else:
                old = m[rows, :]
                new = jnp.maximum(old[:, 0:1], jnp.max(s, axis=1, keepdims=True))
            p = jnp.exp2((s - new) * scale).astype(BF16)
            o = dot(p, v[...])
            if diagonal:
                acc[rows, :] = o
            else:
                acc[rows, :] = acc[rows, :] * jnp.exp2((old[:, 0:1] - new) * scale) + o
            m[rows, :] = jnp.broadcast_to(new, (QT, 128))

    def attend(block, diagonal):
        expand(block)

        def body(i, carry):
            tile(i, diagonal)
            return carry

        lax.fori_loop(0, ROWS // QT, body, 0)

    vs[:, 64:128] = jnp.ones((ROWS, 64), BF16)
    vl[:, 128:256] = jnp.ones((ROWS, 128), BF16)

    local[0].wait()
    lat_event(0)
    local[1].wait()
    res.line(0)
    share_res(0).start()
    attend(sp, True)
    for n in range(1, 12):
        lat_event(n)
        if n <= 3:
            res.line(n)
            share_res((-1, 1, 2)[n - 1]).start()
    local[2].wait()
    w_a.event(0)
    w_b.event(0)
    for rel in others:
        share_lat(rel, 1 - core).wait_recv()
    for dx in (0, -1, 1, 2):
        share_res(dx, 1 - core).wait_recv()

    when = {3: 1, 4: 2, 5: 3, 6: 4, 8: 5, 9: 6, 11: 7, 12: 8, 13: 9, 14: 10, 15: 11}

    def step(t, carry):
        for n, event in when.items():
            @pl.when(t == n)
            def _():
                w_a.event(event)
                w_b.event(event)
        block = lax.rem(z + t // 4, 4) * 4 + lax.rem(y + lax.rem(t, 4), 4)

        @pl.when(block < sp)
        def _():
            attend(block, False)
        return carry

    lax.fori_loop(1, 16, step, 0)

    mine = obuf.at[tp]
    mine[0:ROWS, :] = (acl[:, 0:128] / acl[:, 128:256]).astype(BF16)
    low, high = acs[0:384, :], acs[384:768, :]
    low = low / pltpu.roll(low, 64, 1)
    high = pltpu.roll(high, 64, 1) / high
    left = lax.broadcasted_iota(jnp.int32, (384, 128), 1) < 64
    mine[ROWS:1152, :] = jnp.where(left, low, high).astype(BF16)
    att.line(0)
    share_att(0).start()
    for n in range(1, 4):
        att.line(n)
        share_att((-1, 1, 2)[n - 1]).start()
    for dx in (0, -1, 1, 2):
        share_att(dx, 1 - core).wait_recv()
    for n in range(8):
        abuf[:, 512 + 128 * n : 640 + 128 * n] = obuf[n, 0:ROWS, :]
    for n in range(4):
        one = obuf[2 * n, ROWS:1152, :].astype(F32)
        two = obuf[2 * n + 1, ROWS:1152, :].astype(F32)
        abuf[0:384, 128 * n : 128 * n + 128] = jnp.where(left, one, pltpu.roll(two, 64, 1)).astype(BF16)
        abuf[384:768, 128 * n : 128 * n + 128] = jnp.where(left, pltpu.roll(one, 64, 1), two).astype(BF16)
    local[3].wait()
    res.finish()
    for dx in (0, -1, 1, 2):
        share_res(dx).wait_send()

    def project(i, carry):
        rows = pl.ds(pl.multiple_of(i * MT, MT), MT)
        wide = dot(abuf[rows, :], owbuf[...]) + mid[rows, :].astype(F32)
        middle = wide.astype(BF16)
        mid[rows, :] = middle
        wide = middle.astype(F32)
        scaled = wide * lax.rsqrt(jnp.mean(wide * wide, axis=-1, keepdims=True) + EPSILON)
        nbuf[rows, :] = (scaled * gain_ref[...].astype(F32)).astype(BF16)
        return carry

    lax.fori_loop(0, ROWS // MT, project, 0)

    def hidden(i, carry):
        rows = pl.ds(pl.multiple_of(i * MT, MT), MT)
        both = dot(nbuf[rows, :], wbuf[:, 0 : 2 * FFD])
        gate, upward = both[:, 0:FFD], both[:, FFD:]
        hbuf[rows, :] = (gate / (1.0 + jnp.exp(-gate)) * upward).astype(BF16)
        return carry

    lax.fori_loop(0, ROWS // MT, hidden, 0)

    def swap(n):
        return beside(xs.at[n], xr.at[n], d_s.at[n], d_r.at[n])

    def down(n, carry):
        chip = lax.rem(x + 2 + n * 3, 4)
        rows = pl.ds(pl.multiple_of(chip * 192, 64), 192)
        part = dot(hbuf[rows, :], wbuf[:, 2 * FFD : 3 * FFD], 1, 1).astype(BF16)

        @pl.when(core == 0)
        def _():
            po[n] = part[0:96]
            xs[n] = part[96:192]

        @pl.when(core == 1)
        def _():
            po[n] = part[96:192]
            xs[n] = part[0:96]
        swap(n).start()
        return carry

    lax.fori_loop(0, 4, down, 0)

    def hop(src, dst, to, k):
        return pltpu.make_async_remote_copy(
            src_ref=src, dst_ref=dst, send_sem=f_s.at[k], recv_sem=f_r.at[k],
            device_id=to_x(to, 0), device_id_type=mesh_id,
        )

    def summed(n):
        swap(n).wait_recv()
        return po[n].astype(F32) + xr[n].astype(F32)

    far = summed(0)
    st[0] = far.astype(BF16)
    hops = [
        hop(st.at[0, pl.ds(0, 48)], ra, 1, 0),
        hop(st.at[0, pl.ds(48, 48)], rb, -1, 1),
    ]
    hops[0].start()
    hops[1].start()
    ahead = summed(1)
    st[1, 48:96, :] = ahead[48:96].astype(BF16)
    hops.append(hop(st.at[1, pl.ds(48, 48)], fa.at[pl.ds(48, 48)], 1, 2))
    hops[2].start()
    behind = summed(3)
    st[2, 0:48, :] = behind[0:48].astype(BF16)
    hops.append(hop(st.at[2, pl.ds(0, 48)], fb.at[pl.ds(0, 48)], -1, 3))
    hops[3].start()
    hops[0].wait_recv()
    so[0] = (ahead[0:48] + ra[...].astype(F32)).astype(BF16)
    hops.append(hop(so.at[0], fa.at[pl.ds(0, 48)], 1, 4))
    hops[4].start()
    hops[1].wait_recv()
    so[1] = (behind[48:96] + rb[...].astype(F32)).astype(BF16)
    hops.append(hop(so.at[1], fb.at[pl.ds(48, 48)], -1, 5))
    hops[5].start()
    total = summed(2) + mid[pl.ds(pl.multiple_of(tp * OWN, 32), OWN), :].astype(F32)
    for h in hops[2:]:
        h.wait_recv()
    out_ref[...] = (total + fa[...].astype(F32) + fb[...].astype(F32)).astype(BF16)

    for flow in (lat_a, lat_b, w_a, w_b, att):
        flow.finish()
    for rel in others:
        share_lat(rel).wait_send()
    for dx in (0, -1, 1, 2):
        share_att(dx).wait_send()
    for n in range(4):
        swap(n).wait_send()
    for h in hops:
        h.wait_send()


def on_device(
    resid, query_small, query_large, kv_latent, rope_key, kv_gain, up_key_small, up_value_small,
    up_key_large, up_value_large, out_weight, mix_gain, gate_weight, up_weight, down_weight,
):
    rows = kv_latent.shape[0]
    positions = lax.axis_index("sp") * rows + jnp.arange(rows, dtype=jnp.int32)
    angle_cos, angle_sin = angles(positions, ROTARY)
    latent = norm_rows(kv_latent, kv_gain)
    turned = rotate(rope_key, angle_cos, angle_sin)
    turned = turned.reshape(3, 256, ROTARY).transpose(0, 2, 1).reshape(96, 256)
    lat = jnp.concatenate([latent, turned, jnp.zeros((32, 256), BF16)], axis=0)

    def turn(query, nope):
        return jnp.concatenate(
            [query[:, :nope], rotate(query[:, nope:], angle_cos, angle_sin)], axis=1
        )

    qs = turn(query_small, NOPE_SMALL)
    ql = turn(query_large, NOPE_LARGE)
    wk = jnp.concatenate([up_key_small, up_key_large], axis=1).T
    wv = jnp.concatenate([up_value_large, up_value_small], axis=1)
    w = jnp.concatenate([gate_weight, up_weight, down_weight], axis=1)

    vmem = pl.BlockSpec(memory_space=pltpu.VMEM)
    hbm = pl.BlockSpec(memory_space=pl.ANY)
    dma = pltpu.SemaphoreType.DMA
    return pl.pallas_call(
        kernel,
        out_shape=jax.ShapeDtypeStruct((OWN, D), BF16),
        in_specs=[hbm, vmem, vmem, vmem, vmem, hbm, hbm, vmem, hbm],
        out_specs=vmem,
        scratch_shapes=[
            pltpu.VMEM((16, LAT_ROWS, 256), BF16),
            pltpu.VMEM((D, 3 * FFD), BF16),
            pltpu.VMEM((1536, D), BF16),
            pltpu.VMEM((ROWS, D), BF16),
            pltpu.VMEM((ROWS, D), BF16),
            pltpu.VMEM((8, 1152, 128), BF16),
            pltpu.VMEM((ROWS, 1536), BF16),
            pltpu.VMEM((96, ROWS), BF16),
            pltpu.VMEM((160, ROWS), BF16),
            pltpu.VMEM((ROWS, 128), BF16),
            pltpu.VMEM((ROWS, 256), BF16),
            pltpu.VMEM((ROWS, 128), F32),
            pltpu.VMEM((ROWS, 128), F32),
            pltpu.VMEM((ROWS, 128), F32),
            pltpu.VMEM((ROWS, 256), F32),
            pltpu.VMEM((ROWS, FFD), BF16),
            pltpu.VMEM((4, OWN, D), BF16),
            pltpu.VMEM((4, OWN, D), BF16),
            pltpu.VMEM((4, OWN, D), BF16),
            pltpu.VMEM((48, D), BF16),
            pltpu.VMEM((48, D), BF16),
            pltpu.VMEM((OWN, D), BF16),
            pltpu.VMEM((OWN, D), BF16),
            pltpu.VMEM((3, OWN, D), BF16),
            pltpu.VMEM((2, 48, D), BF16),
            dma((4,)),
            *[dma((20,)) for _ in range(8)],
            dma((16,)), dma((16,)),
            *[dma((4,)) for _ in range(8)],
            dma((4,)), dma((4,)), dma((6,)), dma((6,)),
        ],
        compiler_params=pltpu.CompilerParams(
            collective_id=0, has_side_effects=True, vmem_limit_bytes=67043328
        ),
    )(lat, qs, ql, wk, wv, out_weight, resid, mix_gain.reshape(1, D), w)


def solution(mesh):
    placed = (
        P(("sp", "tp"), None), P("sp", "tp"), P("sp", "tp"), P("sp", None), P("sp", None), P(),
        P(None, "tp"), P(None, "tp"), P(None, "tp"), P(None, "tp"), P(), P(),
        P("sp", "tp"), P("sp", "tp"), P("sp", "tp"),
    )
    return jax.shard_map(
        on_device, mesh=mesh, in_specs=placed, out_specs=P(("sp", "tp"), None), check_vma=False
    )
```

```python
import functools
import math

import jax
import jax.numpy as jnp
from jax import lax
from jax.experimental import pallas as pl
from jax.experimental.pallas import tpu as pltpu
from jax.sharding import PartitionSpec as P

NOPE_SMALL = 64
NOPE_LARGE = 128
ROTARY = 32
THETA = 10000.0
EPSILON = 1e-06
FLOOR = -1e30
ROWS = 768
LAT_ROWS = 896
D = 2048
OWN = 96
FFD = 704
QT = 256
MT = 256
F32 = jnp.float32
BF16 = jnp.bfloat16


def dot(a, b, ca=1, cb=0):
    return lax.dot_general(a, b, (((ca,), (cb,)), ((), ())), preferred_element_type=F32)


class Flow:
    def __init__(self, view, size, send_sem, recv_sem, block, target):
        self.view, self.size = view, size
        self.send_sem, self.recv_sem = send_sem, recv_sem
        self.block, self.target = block, target
        self.sent = []

    def copy(self, at, lo, size, to, k):
        ref = self.view(self.block(*at), lo, size)
        return pltpu.make_async_remote_copy(
            src_ref=ref,
            dst_ref=ref,
            send_sem=self.send_sem.at[k],
            recv_sem=self.recv_sem.at[k],
            device_id=self.target(*to),
            device_id_type=pl.DeviceIdType.MESH,
        )

    def send(self, at, part, to, k):
        lo, size = self.span(part)
        self.sent.append((at, lo, size, to, k))
        self.copy(at, lo, size, to, k).start()

    def span(self, part):
        half = self.size // 2
        return {None: (0, self.size), 0: (0, half), 1: (half, half)}[part]

    def wait(self, at, part, k):
        lo, size = self.span(part)
        self.copy(at, lo, size, (1, 0), k).wait_recv()

    def finish(self):
        for at, lo, size, to, k in self.sent:
            self.copy(at, lo, size, to, k).wait_send()

    def start_u(self):
        self.send((0, 0), None, (1, 0), 0)
        self.send((0, 0), None, (-1, 0), 1)

    def spread(self, du, k):
        self.send((du, 0), None, (0, 1), k)
        self.send((du, 0), None, (0, -1), k + 1)

    def relay_v(self, du, k):
        self.wait((du, -1), None, k)
        self.send((du, -1), 0, (0, 1), k + 2)
        self.wait((du, 1), None, k + 1)
        self.send((du, 1), 1, (0, -1), k + 3)

    def end_v(self, du, k):
        self.wait((du, 2), 0, k + 2)
        self.wait((du, 2), 1, k + 3)

    def event(self, n):
        if n == 0:
            self.start_u()
            self.spread(0, 4)
        elif n == 1:
            self.wait((-1, 0), None, 0)
            self.send((-1, 0), 0, (1, 0), 2)
            self.spread(-1, 8)
        elif n == 2:
            self.wait((1, 0), None, 1)
            self.send((1, 0), 1, (-1, 0), 3)
            self.spread(1, 12)
        elif n == 3:
            self.relay_v(0, 4)
        elif n == 4:
            self.wait((2, 0), 0, 2)
            self.wait((2, 0), 1, 3)
            self.spread(2, 16)
        elif n == 5:
            self.relay_v(-1, 8)
        elif n == 6:
            self.relay_v(1, 12)
        elif n == 7:
            self.relay_v(2, 16)
        else:
            du = (0, -1, 1, 2)[n - 8]
            self.end_v(du, 4 + 4 * (n - 8))

    def line(self, n):
        if n == 0:
            self.start_u()
        elif n == 1:
            self.wait((-1, 0), None, 0)
            self.send((-1, 0), 0, (1, 0), 2)
        elif n == 2:
            self.wait((1, 0), None, 1)
            self.send((1, 0), 1, (-1, 0), 3)
        elif n == 3:
            self.wait((2, 0), 0, 2)
            self.wait((2, 0), 1, 3)


def done_at(du, dv):
    if dv == 0:
        return {0: 0, -1: 1, 1: 2, 2: 4}[du]
    if dv == 2:
        return 8 + (0, -1, 1, 2).index(du)
    return {0: 3, -1: 5, 1: 6, 2: 7}[du]


def kernel(
    lat_ref, rk_ref, trig_ref, kvg_ref, qs_in, ql_in, wks_ref, wkl_ref, wvs_ref, wvl_ref,
    ow_hbm, res_hbm, gain_ref, gate_hbm, up_hbm, down_hbm,
    out_ref,
    lbuf, wbuf, owbuf, mid, nbuf, obuf, abuf, qs_ref, ql_ref, wk_ref, wv_ref, ks, kl, vs, vl,
    ms, ml, acs, acl, hbuf, po, xs, xr, ra, rb, fa, fb, st, so,
    cp, la_s, la_r, lb_s, lb_r, wa_s, wa_r, wb_s, wb_r, ls_s, ls_r,
    r_s, r_r, rs_s, rs_r, o_s, o_r, os_s, os_r, d_s, d_r, f_s, f_r,
):
    sp, tp = lax.axis_index("sp"), lax.axis_index("tp")
    z, y = sp // 4, lax.rem(sp, 4)
    x, core = tp // 2, lax.rem(tp, 2)
    mesh_id = pl.DeviceIdType.MESH

    def at_sp(dy, dz):
        return lax.rem(z + dz + 4, 4) * 4 + lax.rem(y + dy + 4, 4)

    def at_x(dx, _=0):
        return lax.rem(x + dx + 4, 4)

    sibling = {"tp": x * 2 + 1 - core}
    near = [{"sp": at_sp(*d)} for d in ((1, 0), (-1, 0), (0, 1), (0, -1))]
    near += [{"tp": at_x(d) * 2 + core} for d in (1, -1)] + [sibling]

    column = pl.ds(pl.multiple_of(sp * 128, 128), 128)
    local = [
        pltpu.make_async_copy(res_hbm, mid.at[pl.ds(pl.multiple_of(tp * OWN, 32), OWN)], cp.at[0]),
        pltpu.make_async_copy(gate_hbm, wbuf.at[0:FFD, column], cp.at[1]),
        pltpu.make_async_copy(up_hbm, wbuf.at[FFD : 2 * FFD, column], cp.at[2]),
        pltpu.make_async_copy(down_hbm, wbuf.at[2 * FFD : 3 * FFD, column], cp.at[3]),
        pltpu.make_async_copy(ow_hbm, owbuf, cp.at[4]),
    ]
    for c in local:
        c.start()
    barrier = pltpu.get_barrier_semaphore()
    for n in near:
        pl.semaphore_signal(barrier, inc=1, device_id=n, device_id_type=mesh_id)

    trig_cos, trig_sin = trig_ref[0:16, :], trig_ref[16:32, :]

    def turn(first, second):
        first, second = first.astype(F32), second.astype(F32)
        return (
            (first * trig_cos - second * trig_sin).astype(BF16),
            (second * trig_cos + first * trig_sin).astype(BF16),
        )

    wide = lat_ref[...].astype(F32)
    scaled = wide * lax.rsqrt(jnp.mean(wide * wide, axis=-1, keepdims=True) + EPSILON)
    lbuf[sp, 0:ROWS, :] = (scaled * kvg_ref[...].astype(F32)).astype(BF16)
    one, two = turn(rk_ref[0:16, :], rk_ref[16:32, :])
    for n in range(3):
        lbuf[sp, ROWS + 32 * n : ROWS + 32 * n + 16, :] = one[:, 256 * n : 256 * n + 256]
        lbuf[sp, ROWS + 32 * n + 16 : ROWS + 32 * n + 32, :] = two[:, 256 * n : 256 * n + 256]
    lbuf[sp, ROWS + 96 : LAT_ROWS, :] = jnp.zeros((LAT_ROWS - ROWS - 96, 256), BF16)
    pl.semaphore_wait(barrier, len(near))

    q_rows = LAT_ROWS // 4

    def lat_view(piece):
        def view(block, lo, size):
            base = pl.multiple_of((core * 2 + piece) * q_rows, 16)
            return lbuf.at[block, pl.ds(base + lo, size)]
        return view

    def w_view(piece):
        def view(block, lo, size):
            return wbuf.at[
                pl.ds(1056 * piece + lo, size), pl.ds(pl.multiple_of(block * 128, 128), 128)
            ]
        return view

    def yz(du, dv):
        return at_sp(du, dv)

    def zy(du, dv):
        return at_sp(dv, du)

    def to_yz(du, dv):
        return {"sp": at_sp(du, dv)}

    def to_zy(du, dv):
        return {"sp": at_sp(dv, du)}

    def to_x(du, _):
        return {"tp": at_x(du) * 2 + core}

    lat_a = Flow(lat_view(0), q_rows, la_s, la_r, yz, to_yz)
    lat_b = Flow(lat_view(1), q_rows, lb_s, lb_r, zy, to_zy)
    w_a = Flow(w_view(0), 1056, wa_s, wa_r, yz, to_yz)
    w_b = Flow(w_view(1), 1056, wb_s, wb_r, zy, to_zy)

    def res_view(chip, lo, size, c=None):
        c = core if c is None else c
        return mid.at[pl.ds(pl.multiple_of((chip * 2 + c) * OWN, 32) + lo, size)]

    def o_view(chip, lo, size, c=None):
        c = core if c is None else c
        return obuf.at[chip * 2 + c, pl.ds(lo, size)]

    res = Flow(res_view, OWN, r_s, r_r, at_x, to_x)
    att = Flow(o_view, 1152, o_s, o_r, at_x, to_x)

    def beside(src, dst, s, r):
        return pltpu.make_async_remote_copy(
            src_ref=src, dst_ref=dst, send_sem=s, recv_sem=r, device_id=sibling, device_id_type=mesh_id
        )

    def share_lat(rel, c=None):
        base = pl.multiple_of((core if c is None else c) * (2 * q_rows), 64)
        ref = lbuf.at[at_sp(*rel), pl.ds(base, 2 * q_rows)]
        n = (rel[1] % 4) * 4 + rel[0] % 4
        return beside(ref, ref, ls_s.at[n], ls_r.at[n])

    def share_line(view, size, s, r, dx, c=None):
        ref = view(at_x(dx), 0, size, c)
        return beside(ref, ref, s.at[dx % 4], r.at[dx % 4])

    share_res = functools.partial(share_line, res_view, OWN, rs_s, rs_r)
    share_att = functools.partial(share_line, o_view, 1152, os_s, os_r)

    others = [
        (-1, 0), (1, 0), (0, -1), (0, 1), (-1, -1), (-1, 1), (1, -1), (1, 1),
        (2, 0), (0, 2), (2, -1), (-1, 2), (2, 1), (1, 2), (2, 2),
    ]

    def lat_event(n):
        lat_a.event(n)
        lat_b.event(n)
        for rel in others:
            if max(done_at(*rel), done_at(rel[1], rel[0])) == n:
                share_lat(rel).start()

    scale_small = math.log2(math.e) / math.sqrt(NOPE_SMALL + ROTARY)
    scale_large = math.log2(math.e) / math.sqrt(NOPE_LARGE + ROTARY)

    def expand(block):
        latent = lbuf[block, 0:ROWS, :]
        keys = dot(latent, wk_ref[...]).astype(BF16)
        kl[:, 0:128] = keys[:, 0:128]
        ks[:, 0:64] = keys[:, 128:192]
        for n in range(3):
            turned = lbuf[block, ROWS + 32 * n : ROWS + 32 * n + 32, :]
            turned = turned.astype(F32).T.astype(BF16)
            ks[256 * n : 256 * n + 256, 64:96] = turned
            kl[256 * n : 256 * n + 256, 128:160] = turned
        values = dot(wv_ref[...], latent, 1, 1).astype(BF16)
        vl[0:128, :] = values[0:128]
        vs[0:64, :] = values[128:192]

    heads = (
        (ql_ref, kl, vl, ml, acl, scale_large),
        (qs_ref, ks, vs, ms, acs, scale_small),
    )

    def attend(block, diagonal):
        expand(block)
        units = [(i, h) for i in range(ROWS // QT) for h in heads]
        scores, soft = {}, {}

        def score(u):
            i, (q, k, *_) = units[u]
            scores[u] = dot(k[...], q[:, i * QT : i * QT + QT])

        def weigh(u):
            i, (_, _, _, m, _, scale) = units[u]
            s, cols = scores.pop(u), slice(i * QT, i * QT + QT)
            if diagonal:
                row = lax.broadcasted_iota(jnp.int32, (ROWS, QT), 0)
                col = lax.broadcasted_iota(jnp.int32, (ROWS, QT), 1) + i * QT
                s = jnp.where(row <= col, s, FLOOR)
                new = jnp.max(s, axis=0, keepdims=True)
                fade = None
            else:
                old = m[:, cols]
                new = jnp.maximum(old, jnp.max(s, axis=0, keepdims=True))
                fade = jnp.exp2((old - new) * scale)
            m[:, cols] = new
            soft[u] = (jnp.exp2((s - new) * scale).astype(BF16), fade)

        def gather(u):
            i, (_, _, v, _, acc, _) = units[u]
            (p, fade), cols = soft.pop(u), slice(i * QT, i * QT + QT)
            o = dot(v[...], p)
            acc[:, cols] = o if diagonal else acc[:, cols] * fade + o

        score(0)
        score(1)
        for u in range(len(units)):
            if u + 2 < len(units):
                score(u + 2)
            weigh(u)
            if u > 0:
                gather(u - 1)
        gather(len(units) - 1)

    lat_event(0)
    local[0].wait()
    res.line(0)
    share_res(0).start()

    for inp, ref, nope in ((qs_in, qs_ref, NOPE_SMALL), (ql_in, ql_ref, NOPE_LARGE)):
        ref[0:nope, :] = inp[0:nope, :]
        one, two = turn(inp[nope : nope + 16, :], inp[nope + 16 : nope + 32, :])
        ref[nope : nope + 16, :] = one
        ref[nope + 16 : nope + 32, :] = two
    wk_ref[:, 0:128] = wkl_ref[...]
    wk_ref[:, 128:192] = wks_ref[...].astype(F32).T.astype(BF16)
    wv_ref[0:128, :] = wvl_ref[...].astype(F32).T.astype(BF16)
    wv_ref[128:192, :] = wvs_ref[...]
    vs[64:80, :] = jnp.ones((16, ROWS), BF16)
    vl[128:144, :] = jnp.ones((16, ROWS), BF16)

    attend(sp, True)
    for n in range(1, 3):
        lat_event(n)
        res.line(n)
        share_res((-1, 1)[n - 1]).start()
    for c in local[1:4]:
        c.wait()

    def w_event(n):
        w_a.event(n)
        w_b.event(n)

    def w_first(n):
        for w in (w_a, w_b):
            w.start_u() if n == 0 else w.spread(0, 4)

    todo = {t: [] for t in range(1, 17)}
    todo[1] += [(lat_event, 3), (res.line, 3), (lambda n: share_res(2).start(), 0)]
    for t in range(2, 9):
        todo[t].append((lat_event, t + 2))
    todo[9].append((lat_event, 11))
    todo[2].append((w_first, 0))
    todo[6].append((w_first, 1))
    for t, n in ((10, 1), (11, 2), (12, 3), (13, 4), (14, 5), (15, 6)):
        todo[t].append((w_event, n))
    todo[16] = [(w_event, n) for n in range(7, 12)]
    for t, rel in enumerate(others):
        todo[t + 1].append((lambda r: share_lat(r, 1 - core).wait_recv(), rel))

    def step(t, carry):
        dy, dz = 0, 0
        for n in range(1, 16):
            dy = jnp.where(t == n, others[n - 1][0], dy)
            dz = jnp.where(t == n, others[n - 1][1], dz)

            @pl.when(t == n)
            def _():
                for what, arg in todo[n]:
                    what(arg)
        block = at_sp(dy, dz)

        @pl.when(block < sp)
        def _():
            attend(block, False)
        return carry

    lax.fori_loop(1, 16, step, 0)
    for dx in (0, -1, 1, 2):
        share_res(dx, 1 - core).wait_recv()

    mine = obuf.at[tp]
    mine[0:ROWS, :] = (acl[0:128, :] / acl[128:129, :]).T.astype(BF16)
    small = acs[0:64, :] / acs[64:65, :]
    small = jnp.concatenate([small[:, 0:384], small[:, 384:768]], axis=0)
    mine[ROWS:1152, :] = small.T.astype(BF16)
    left = lax.broadcasted_iota(jnp.int32, (384, 128), 1) < 64
    att.line(0)
    share_att(0).start()
    for n in range(1, 4):
        att.line(n)
        share_att((-1, 1, 2)[n - 1]).start()
    for dx in (0, -1, 1, 2):
        share_att(dx, 1 - core).wait_recv()
    for n in range(8):
        abuf[:, 512 + 128 * n : 640 + 128 * n] = obuf[n, 0:ROWS, :]
    for n in range(4):
        one = obuf[2 * n, ROWS:1152, :].astype(F32)
        two = obuf[2 * n + 1, ROWS:1152, :].astype(F32)
        abuf[0:384, 128 * n : 128 * n + 128] = jnp.where(left, one, pltpu.roll(two, 64, 1)).astype(BF16)
        abuf[384:768, 128 * n : 128 * n + 128] = jnp.where(left, pltpu.roll(one, 64, 1), two).astype(BF16)
    local[4].wait()
    res.finish()
    for dx in (0, -1, 1, 2):
        share_res(dx).wait_send()

    def project(i, carry):
        rows = pl.ds(pl.multiple_of(i * MT, MT), MT)
        wide = dot(abuf[rows, :], owbuf[...]) + mid[rows, :].astype(F32)
        middle = wide.astype(BF16)
        mid[rows, :] = middle
        wide = middle.astype(F32)
        scaled = wide * lax.rsqrt(jnp.mean(wide * wide, axis=-1, keepdims=True) + EPSILON)
        nbuf[rows, :] = (scaled * gain_ref[...].astype(F32)).astype(BF16)
        return carry

    lax.fori_loop(0, ROWS // MT, project, 0)
    for what, arg in todo[16]:
        what(arg)

    def hidden(i, carry):
        rows = pl.ds(pl.multiple_of(i * MT, MT), MT)
        both = dot(wbuf[0 : 2 * FFD, :], nbuf[rows, :], 1, 1)
        gate, upward = both[0:FFD], both[FFD:]
        hbuf[rows, :] = (gate / (1.0 + jnp.exp(-gate)) * upward).T.astype(BF16)
        return carry

    lax.fori_loop(0, ROWS // MT, hidden, 0)

    def swap(n):
        return beside(xs.at[n], xr.at[n], d_s.at[n], d_r.at[n])

    def down(n, carry):
        chip = lax.rem(x + 2 + n * 3, 4)
        rows = pl.ds(pl.multiple_of(chip * 192, 64), 192)
        part = dot(hbuf[rows, :], wbuf[2 * FFD : 3 * FFD, :]).astype(BF16)

        @pl.when(core == 0)
        def _():
            po[n] = part[0:96]
            xs[n] = part[96:192]

        @pl.when(core == 1)
        def _():
            po[n] = part[96:192]
            xs[n] = part[0:96]
        swap(n).start()
        return carry

    lax.fori_loop(0, 4, down, 0)

    def hop(src, dst, to, k):
        return pltpu.make_async_remote_copy(
            src_ref=src, dst_ref=dst, send_sem=f_s.at[k], recv_sem=f_r.at[k],
            device_id=to_x(to, 0), device_id_type=mesh_id,
        )

    def summed(n):
        swap(n).wait_recv()
        return po[n].astype(F32) + xr[n].astype(F32)

    far = summed(0)
    st[0] = far.astype(BF16)
    hops = [
        hop(st.at[0, pl.ds(0, 48)], ra, 1, 0),
        hop(st.at[0, pl.ds(48, 48)], rb, -1, 1),
    ]
    hops[0].start()
    hops[1].start()
    ahead = summed(1)
    st[1, 48:96, :] = ahead[48:96].astype(BF16)
    hops.append(hop(st.at[1, pl.ds(48, 48)], fa.at[pl.ds(48, 48)], 1, 2))
    hops[2].start()
    behind = summed(3)
    st[2, 0:48, :] = behind[0:48].astype(BF16)
    hops.append(hop(st.at[2, pl.ds(0, 48)], fb.at[pl.ds(0, 48)], -1, 3))
    hops[3].start()
    hops[0].wait_recv()
    so[0] = (ahead[0:48] + ra[...].astype(F32)).astype(BF16)
    hops.append(hop(so.at[0], fa.at[pl.ds(0, 48)], 1, 4))
    hops[4].start()
    hops[1].wait_recv()
    so[1] = (behind[48:96] + rb[...].astype(F32)).astype(BF16)
    hops.append(hop(so.at[1], fb.at[pl.ds(48, 48)], -1, 5))
    hops[5].start()
    total = summed(2) + mid[pl.ds(pl.multiple_of(tp * OWN, 32), OWN), :].astype(F32)
    for h in hops[2:]:
        h.wait_recv()
    out_ref[...] = (total + fa[...].astype(F32) + fb[...].astype(F32)).astype(BF16)

    for flow in (lat_a, lat_b, w_a, w_b, att):
        flow.finish()
    for rel in others:
        share_lat(rel).wait_send()
    for dx in (0, -1, 1, 2):
        share_att(dx).wait_send()
    for n in range(4):
        swap(n).wait_send()
    for h in hops:
        h.wait_send()


def on_device(
    resid, query_small, query_large, kv_latent, rope_key, kv_gain, up_key_small, up_value_small,
    up_key_large, up_value_large, out_weight, mix_gain, gate_weight, up_weight, down_weight,
):
    rows = kv_latent.shape[0]
    positions = lax.axis_index("sp") * rows + jnp.arange(rows, dtype=jnp.int32)
    inverse = THETA ** (-jnp.arange(0, ROTARY, 2).astype(F32) / ROTARY)
    phase = inverse[:, None] * positions.astype(F32)[None, :]
    trig = jnp.concatenate([jnp.cos(phase), jnp.sin(phase)], axis=0)

    vmem = pl.BlockSpec(memory_space=pltpu.VMEM)
    hbm = pl.BlockSpec(memory_space=pl.ANY)
    dma = pltpu.SemaphoreType.DMA
    return pl.pallas_call(
        kernel,
        out_shape=jax.ShapeDtypeStruct((OWN, D), BF16),
        in_specs=[vmem] * 10 + [hbm, hbm, vmem, hbm, hbm, hbm],
        out_specs=vmem,
        scratch_shapes=[
            pltpu.VMEM((16, LAT_ROWS, 256), BF16),
            pltpu.VMEM((3 * FFD, D), BF16),
            pltpu.VMEM((1536, D), BF16),
            pltpu.VMEM((ROWS, D), BF16),
            pltpu.VMEM((ROWS, D), BF16),
            pltpu.VMEM((8, 1152, 128), BF16),
            pltpu.VMEM((ROWS, 1536), BF16),
            pltpu.VMEM((96, ROWS), BF16),
            pltpu.VMEM((160, ROWS), BF16),
            pltpu.VMEM((256, 192), BF16),
            pltpu.VMEM((192, 256), BF16),
            pltpu.VMEM((ROWS, 96), BF16),
            pltpu.VMEM((ROWS, 160), BF16),
            pltpu.VMEM((80, ROWS), BF16),
            pltpu.VMEM((144, ROWS), BF16),
            pltpu.VMEM((1, ROWS), F32),
            pltpu.VMEM((1, ROWS), F32),
            pltpu.VMEM((80, ROWS), F32),
            pltpu.VMEM((144, ROWS), F32),
            pltpu.VMEM((ROWS, FFD), BF16),
            pltpu.VMEM((4, OWN, D), BF16),
            pltpu.VMEM((4, OWN, D), BF16),
            pltpu.VMEM((4, OWN, D), BF16),
            pltpu.VMEM((48, D), BF16),
            pltpu.VMEM((48, D), BF16),
            pltpu.VMEM((OWN, D), BF16),
            pltpu.VMEM((OWN, D), BF16),
            pltpu.VMEM((3, OWN, D), BF16),
            pltpu.VMEM((2, 48, D), BF16),
            dma((5,)),
            *[dma((20,)) for _ in range(8)],
            dma((16,)), dma((16,)),
            *[dma((4,)) for _ in range(8)],
            dma((4,)), dma((4,)), dma((6,)), dma((6,)),
        ],
        compiler_params=pltpu.CompilerParams(
            collective_id=0, has_side_effects=True, vmem_limit_bytes=67043328
        ),
    )(
        kv_latent, rope_key.T, trig, kv_gain.reshape(1, 256), query_small.T, query_large.T,
        up_key_small.T, up_key_large, up_value_small.T, up_value_large,
        out_weight, resid, mix_gain.reshape(1, D), gate_weight.T, up_weight.T, down_weight.T,
    )


def solution(mesh):
    placed = (
        P(("sp", "tp"), None), P("sp", "tp"), P("sp", "tp"), P("sp", None), P("sp", None), P(),
        P(None, "tp"), P(None, "tp"), P(None, "tp"), P(None, "tp"), P(), P(),
        P("sp", "tp"), P("sp", "tp"), P("sp", "tp"),
    )
    return jax.shard_map(
        on_device, mesh=mesh, in_specs=placed, out_specs=P(("sp", "tp"), None), check_vma=False
    )
```

```python
import functools
import math

import jax
import jax.numpy as jnp
from jax import lax
from jax.experimental import pallas as pl
from jax.experimental.pallas import tpu as pltpu
from jax.sharding import PartitionSpec as P

NOPE_SMALL = 64
NOPE_LARGE = 128
ROTARY = 32
THETA = 10000.0
EPSILON = 1e-06
FLOOR = -1e30
ROWS = 768
LAT_ROWS = 896
D = 2048
OWN = 96
FFD = 704
QT = 256
MT = 256
F32 = jnp.float32
BF16 = jnp.bfloat16


def dot(a, b, ca=1, cb=0):
    return lax.dot_general(a, b, (((ca,), (cb,)), ((), ())), preferred_element_type=F32)


class Flow:
    def __init__(self, view, size, send_sem, recv_sem, block, target):
        self.view, self.size = view, size
        self.send_sem, self.recv_sem = send_sem, recv_sem
        self.block, self.target = block, target
        self.sent = []

    def copy(self, at, lo, size, to, k):
        ref = self.view(self.block(*at), lo, size)
        return pltpu.make_async_remote_copy(
            src_ref=ref,
            dst_ref=ref,
            send_sem=self.send_sem.at[k],
            recv_sem=self.recv_sem.at[k],
            device_id=self.target(*to),
            device_id_type=pl.DeviceIdType.MESH,
        )

    def send(self, at, part, to, k):
        lo, size = self.span(part)
        self.sent.append((at, lo, size, to, k))
        self.copy(at, lo, size, to, k).start()

    def span(self, part):
        half = self.size // 2
        return {None: (0, self.size), 0: (0, half), 1: (half, half)}[part]

    def wait(self, at, part, k):
        lo, size = self.span(part)
        self.copy(at, lo, size, (1, 0), k).wait_recv()

    def finish(self):
        for at, lo, size, to, k in self.sent:
            self.copy(at, lo, size, to, k).wait_send()

    def start_u(self):
        self.send((0, 0), None, (1, 0), 0)
        self.send((0, 0), None, (-1, 0), 1)

    def spread(self, du, k):
        self.send((du, 0), None, (0, 1), k)
        self.send((du, 0), None, (0, -1), k + 1)

    def relay_v(self, du, k):
        self.wait((du, -1), None, k)
        self.send((du, -1), 0, (0, 1), k + 2)
        self.wait((du, 1), None, k + 1)
        self.send((du, 1), 1, (0, -1), k + 3)

    def end_v(self, du, k):
        self.wait((du, 2), 0, k + 2)
        self.wait((du, 2), 1, k + 3)

    def event(self, n):
        if n == 0:
            self.start_u()
            self.spread(0, 4)
        elif n == 1:
            self.wait((-1, 0), None, 0)
            self.send((-1, 0), 0, (1, 0), 2)
            self.spread(-1, 8)
        elif n == 2:
            self.wait((1, 0), None, 1)
            self.send((1, 0), 1, (-1, 0), 3)
            self.spread(1, 12)
        elif n == 3:
            self.relay_v(0, 4)
        elif n == 4:
            self.wait((2, 0), 0, 2)
            self.wait((2, 0), 1, 3)
            self.spread(2, 16)
        elif n == 5:
            self.relay_v(-1, 8)
        elif n == 6:
            self.relay_v(1, 12)
        elif n == 7:
            self.relay_v(2, 16)
        else:
            du = (0, -1, 1, 2)[n - 8]
            self.end_v(du, 4 + 4 * (n - 8))

    def line(self, n):
        if n == 0:
            self.start_u()
        elif n == 1:
            self.wait((-1, 0), None, 0)
            self.send((-1, 0), 0, (1, 0), 2)
        elif n == 2:
            self.wait((1, 0), None, 1)
            self.send((1, 0), 1, (-1, 0), 3)
        elif n == 3:
            self.wait((2, 0), 0, 2)
            self.wait((2, 0), 1, 3)


def done_at(du, dv):
    if dv == 0:
        return {0: 0, -1: 1, 1: 2, 2: 4}[du]
    if dv == 2:
        return 8 + (0, -1, 1, 2).index(du)
    return {0: 3, -1: 5, 1: 6, 2: 7}[du]


def kernel(
    lat_ref, rk_ref, trig_ref, gain_ref, qs_in, ql_in, wks_ref, wkl_ref, wvs_ref, wvl_ref,
    ow_hbm, res_hbm, gate_hbm, up_hbm, down_hbm,
    out_ref,
    lbuf, wbuf, owbuf, mid, nbuf, obuf, abuf, qs_ref, ql_ref, wk_ref, wv_ref, ks, kl, vs, vl,
    ms, ml, acs, acl, po, xs, xr, ra, rb, fa, fb, st, so,
    cp, la_s, la_r, wa_s, wa_r, wb_s, wb_r, lb_s, lb_r, ls_s, ls_r,
    r_s, r_r, rs_s, rs_r, o_s, o_r, os_s, os_r, d_s, d_r, f_s, f_r,
):
    sp, tp = lax.axis_index("sp"), lax.axis_index("tp")
    z, y = sp // 4, lax.rem(sp, 4)
    x, core = tp // 2, lax.rem(tp, 2)
    mesh_id = pl.DeviceIdType.MESH

    def at_sp(dy, dz):
        return lax.rem(z + dz + 4, 4) * 4 + lax.rem(y + dy + 4, 4)

    def at_x(dx, _=0):
        return lax.rem(x + dx + 4, 4)

    sibling = {"tp": x * 2 + 1 - core}
    near = [{"sp": at_sp(*d)} for d in ((1, 0), (-1, 0), (0, 1), (0, -1))]
    near += [{"tp": at_x(d) * 2 + core} for d in (1, -1)] + [sibling]

    column = pl.ds(pl.multiple_of(sp * 128, 128), 128)
    local = [
        pltpu.make_async_copy(res_hbm, mid.at[pl.ds(pl.multiple_of(tp * OWN, 32), OWN)], cp.at[0]),
        pltpu.make_async_copy(gate_hbm, wbuf.at[0:FFD, column], cp.at[1]),
        pltpu.make_async_copy(up_hbm, wbuf.at[FFD : 2 * FFD, column], cp.at[2]),
        pltpu.make_async_copy(down_hbm, wbuf.at[2 * FFD : 3 * FFD, column], cp.at[3]),
        pltpu.make_async_copy(ow_hbm, owbuf, cp.at[4]),
    ]
    for c in local:
        c.start()
    barrier = pltpu.get_barrier_semaphore()
    for n in near:
        pl.semaphore_signal(barrier, inc=1, device_id=n, device_id_type=mesh_id)

    trig_cos, trig_sin = trig_ref[0:16, :], trig_ref[16:32, :]

    def turn(first, second):
        first, second = first.astype(F32), second.astype(F32)
        return (
            (first * trig_cos - second * trig_sin).astype(BF16),
            (second * trig_cos + first * trig_sin).astype(BF16),
        )

    wide = lat_ref[...].astype(F32)
    scaled = wide * lax.rsqrt(jnp.mean(wide * wide, axis=-1, keepdims=True) + EPSILON)
    lbuf[sp, 0:ROWS, :] = (scaled * gain_ref[:, 0:256].astype(F32)).astype(BF16)
    one, two = turn(rk_ref[0:16, :], rk_ref[16:32, :])
    for n in range(3):
        lbuf[sp, ROWS + 32 * n : ROWS + 32 * n + 16, :] = one[:, 256 * n : 256 * n + 256]
        lbuf[sp, ROWS + 32 * n + 16 : ROWS + 32 * n + 32, :] = two[:, 256 * n : 256 * n + 256]
    lbuf[sp, ROWS + 96 : LAT_ROWS, :] = jnp.zeros((LAT_ROWS - ROWS - 96, 256), BF16)
    pl.semaphore_wait(barrier, len(near))

    q_rows = LAT_ROWS // 4

    def lat_ref_of(block, far, c, lo=0, size=q_rows):
        base = (2 * lax.rem(x + far, 2) + c) * q_rows + lo
        return lbuf.at[block, pl.ds(pl.multiple_of(base, 16), size)]

    def lat_view(block, lo, size):
        return lat_ref_of(block, 0, core, lo, size)

    def w_view(piece):
        def view(block, lo, size):
            return wbuf.at[
                pl.ds(1056 * piece + lo, size), pl.ds(pl.multiple_of(block * 128, 128), 128)
            ]
        return view

    def yz(du, dv):
        return at_sp(du, dv)

    def zy(du, dv):
        return at_sp(dv, du)

    def to_yz(du, dv):
        return {"sp": at_sp(du, dv)}

    def to_zy(du, dv):
        return {"sp": at_sp(dv, du)}

    def to_x(du, _):
        return {"tp": at_x(du) * 2 + core}

    def by_core(du, dv):
        return at_sp(jnp.where(core == 0, du, dv), jnp.where(core == 0, dv, du))

    lat = Flow(lat_view, q_rows, la_s, la_r, by_core, lambda du, dv: {"sp": by_core(du, dv)})
    w_a = Flow(w_view(0), 1056, wa_s, wa_r, yz, to_yz)
    w_b = Flow(w_view(1), 1056, wb_s, wb_r, zy, to_zy)

    def res_view(chip, lo, size, c=None):
        c = core if c is None else c
        return mid.at[pl.ds(pl.multiple_of((chip * 2 + c) * OWN, 32) + lo, size)]

    def o_view(chip, lo, size, c=None):
        c = core if c is None else c
        return obuf.at[chip * 2 + c, pl.ds(lo, size)]

    res = Flow(res_view, OWN, r_s, r_r, at_x, to_x)
    att = Flow(o_view, 1152, o_s, o_r, at_x, to_x)

    def beside(src, dst, s, r):
        return pltpu.make_async_remote_copy(
            src_ref=src, dst_ref=dst, send_sem=s, recv_sem=r, device_id=sibling, device_id_type=mesh_id
        )

    def number(du, dv):
        return (dv % 4) * 4 + du % 4

    def number_by_core(du, dv):
        return jnp.where(core == 0, number(du, dv), number(dv, du))

    def share_lat(rel, far):
        ref = lat_ref_of(by_core(*rel), far, core)
        n = number_by_core(*rel)
        return beside(ref, ref, ls_s.at[far, n], ls_r.at[far, n])

    def shared_lat(rel, far):
        ref = lat_ref_of(at_sp(*rel), far, 1 - core)
        n = number(*rel)
        return beside(ref, ref, ls_s.at[far, n], ls_r.at[far, n])

    def cross(rel, dx, far=0):
        half = 0 if dx == 1 else 1
        ref = lat_ref_of(by_core(*rel), far, core, half * (q_rows // 2), q_rows // 2)
        n = number(*rel)
        return pltpu.make_async_remote_copy(
            src_ref=ref, dst_ref=ref, send_sem=lb_s.at[half, n], recv_sem=lb_r.at[half, n],
            device_id=to_x(dx, 0), device_id_type=mesh_id,
        )

    def share_line(view, size, s, r, dx, c=None):
        ref = view(at_x(dx), 0, size, c)
        return beside(ref, ref, s.at[dx % 4], r.at[dx % 4])

    share_res = functools.partial(share_line, res_view, OWN, rs_s, rs_r)
    share_att = functools.partial(share_line, o_view, 1152, os_s, os_r)

    others = [
        (-1, 0), (1, 0), (0, -1), (0, 1), (-1, -1), (-1, 1), (1, -1), (1, 1),
        (2, 0), (0, 2), (2, -1), (-1, 2), (2, 1), (1, 2), (2, 2),
    ]

    def lat_event(n):
        lat.event(n)
        for rel in others:
            if done_at(*rel) == n:
                cross(rel, 1).start()
                cross(rel, -1).start()
                share_lat(rel, 0).start()

    def lat_crossed(rel):
        cross(rel, 1, 1).wait_recv()
        cross(rel, -1, 1).wait_recv()
        share_lat(rel, 1).start()

    scale_small = math.log2(math.e) / math.sqrt(NOPE_SMALL + ROTARY)
    scale_large = math.log2(math.e) / math.sqrt(NOPE_LARGE + ROTARY)

    def expand(block):
        latent = lbuf[block, 0:ROWS, :]
        keys = dot(latent, wk_ref[...]).astype(BF16)
        kl[:, 0:128] = keys[:, 0:128]
        ks[:, 0:64] = keys[:, 128:192]
        for n in range(3):
            turned = lbuf[block, ROWS + 32 * n : ROWS + 32 * n + 32, :]
            turned = turned.astype(F32).T.astype(BF16)
            ks[256 * n : 256 * n + 256, 64:96] = turned
            kl[256 * n : 256 * n + 256, 128:160] = turned
        values = dot(wv_ref[...], latent, 1, 1).astype(BF16)
        vl[0:128, :] = values[0:128]
        vs[0:64, :] = values[128:192]

    heads = (
        (ql_ref, kl, vl, ml, acl, scale_large),
        (qs_ref, ks, vs, ms, acs, scale_small),
    )

    def attend(block, diagonal):
        expand(block)
        units = [(i, h) for i in range(ROWS // QT) for h in heads]
        scores, soft = {}, {}

        def score(u):
            i, (q, k, *_) = units[u]
            scores[u] = dot(k[...], q[:, i * QT : i * QT + QT])

        def weigh(u):
            i, (_, _, _, m, _, scale) = units[u]
            s, cols = scores.pop(u), slice(i * QT, i * QT + QT)
            if diagonal:
                row = lax.broadcasted_iota(jnp.int32, (ROWS, QT), 0)
                col = lax.broadcasted_iota(jnp.int32, (ROWS, QT), 1) + i * QT
                s = jnp.where(row <= col, s, FLOOR)
                new = jnp.max(s, axis=0, keepdims=True)
                fade = None
            else:
                old = m[:, cols]
                new = jnp.maximum(old, jnp.max(s, axis=0, keepdims=True))
                fade = jnp.exp2((old - new) * scale)
            m[:, cols] = new
            soft[u] = (jnp.exp2((s - new) * scale).astype(BF16), fade)

        def gather(u):
            i, (_, _, v, _, acc, _) = units[u]
            (p, fade), cols = soft.pop(u), slice(i * QT, i * QT + QT)
            o = dot(v[...], p)
            acc[:, cols] = o if diagonal else acc[:, cols] * fade + o

        score(0)
        score(1)
        for u in range(len(units)):
            if u + 2 < len(units):
                score(u + 2)
            weigh(u)
            if u > 0:
                gather(u - 1)
        gather(len(units) - 1)

    lat_event(0)
    local[0].wait()

    for inp, ref, nope in ((qs_in, qs_ref, NOPE_SMALL), (ql_in, ql_ref, NOPE_LARGE)):
        ref[0:nope, :] = inp[0:nope, :]
        one, two = turn(inp[nope : nope + 16, :], inp[nope + 16 : nope + 32, :])
        ref[nope : nope + 16, :] = one
        ref[nope + 16 : nope + 32, :] = two
    wk_ref[:, 0:128] = wkl_ref[...]
    wk_ref[:, 128:192] = wks_ref[...].astype(F32).T.astype(BF16)
    wv_ref[0:128, :] = wvl_ref[...].astype(F32).T.astype(BF16)
    wv_ref[128:192, :] = wvs_ref[...]
    vs[64:80, :] = jnp.ones((16, ROWS), BF16)
    vl[128:144, :] = jnp.ones((16, ROWS), BF16)

    attend(sp, True)
    for n in range(1, 4):
        lat_event(n)
    for c in local[1:4]:
        c.wait()

    def w_event(n):
        w_a.event(n)
        w_b.event(n)

    def w_first(n):
        for w in (w_a, w_b):
            w.start_u() if n == 0 else w.spread(0, 4)

    def res_event(n):
        res.line(n)
        share_res((0, -1, 1, 2)[n]).start()

    order = sorted(others, key=lambda rel: done_at(*rel))
    todo = {t: [] for t in range(1, 16)}
    todo[1] += [(lat_event, 4), (w_first, 0)]
    todo[1] += [(lat_crossed, order[n]) for n in range(4)]
    todo[2] += [(lat_event, 5), (lat_event, 6), (lat_crossed, order[4])]
    todo[3] += [(lat_event, 7), (lat_event, 8), (w_first, 1), (lat_crossed, order[5]), (lat_crossed, order[6])]
    todo[4] += [(lat_event, 9), (lat_event, 10), (lat_event, 11), (lat_crossed, order[7]), (lat_crossed, order[8])]
    todo[5] += [(lat_crossed, order[9]), (lat_crossed, order[10])]
    todo[6] += [(lat_crossed, order[11]), (lat_crossed, order[12]), (res_event, 0)]
    todo[7] += [(lat_crossed, order[13]), (lat_crossed, order[14])]
    for t, n in ((8, 1), (9, 2), (10, 3)):
        todo[t].append((res_event, n))
    for t, n in ((8, 1), (9, 2), (10, 3)):
        todo[t].append((w_event, n))
    for t, rel in enumerate(others):
        todo[t + 1].append((lambda r: shared_lat(r, 0).wait_recv(), rel))
        todo[t + 1].append((lambda r: shared_lat(r, 1).wait_recv(), rel))

    def step(t, carry):
        dy, dz = 0, 0
        for n in range(1, 16):
            dy = jnp.where(t == n, others[n - 1][0], dy)
            dz = jnp.where(t == n, others[n - 1][1], dz)

            @pl.when(t == n)
            def _():
                for what, arg in todo[n]:
                    what(arg)
        block = at_sp(dy, dz)

        @pl.when(block < sp)
        def _():
            attend(block, False)
        return carry

    lax.fori_loop(1, 16, step, 0)
    for dx in (0, -1, 1, 2):
        share_res(dx, 1 - core).wait_recv()

    mine = obuf.at[tp]
    mine[0:ROWS, :] = (acl[0:128, :] / acl[128:129, :]).T.astype(BF16)
    small = acs[0:64, :] / acs[64:65, :]
    small = jnp.concatenate([small[:, 0:384], small[:, 384:768]], axis=0)
    mine[ROWS:1152, :] = small.T.astype(BF16)
    left = lax.broadcasted_iota(jnp.int32, (384, 128), 1) < 64
    att.line(0)
    share_att(0).start()
    w_event(4)
    for n in range(1, 4):
        att.line(n)
        share_att((-1, 1, 2)[n - 1]).start()
        w_event(4 + n)
    for dx in (0, -1, 1, 2):
        share_att(dx, 1 - core).wait_recv()
    for n in range(8):
        abuf[:, 512 + 128 * n : 640 + 128 * n] = obuf[n, 0:ROWS, :]
    for n in range(4):
        one = obuf[2 * n, ROWS:1152, :].astype(F32)
        two = obuf[2 * n + 1, ROWS:1152, :].astype(F32)
        abuf[0:384, 128 * n : 128 * n + 128] = jnp.where(left, one, pltpu.roll(two, 64, 1)).astype(BF16)
        abuf[384:768, 128 * n : 128 * n + 128] = jnp.where(left, pltpu.roll(one, 64, 1), two).astype(BF16)
    local[4].wait()
    res.finish()
    for dx in (0, -1, 1, 2):
        share_res(dx).wait_send()

    def project(i, carry):
        for n in range(3):
            @pl.when(i == n)
            def _():
                w_event(8 + n)
        rows = pl.ds(pl.multiple_of(i * MT, MT), MT)
        wide = dot(abuf[rows, :], owbuf[...]) + mid[rows, :].astype(F32)
        middle = wide.astype(BF16)
        mid[rows, :] = middle
        wide = middle.astype(F32)
        scaled = wide * lax.rsqrt(jnp.mean(wide * wide, axis=-1, keepdims=True) + EPSILON)
        nbuf[rows, :] = (scaled * gain_ref[:, 256:].astype(F32)).astype(BF16)
        return carry

    lax.fori_loop(0, ROWS // MT, project, 0)
    w_event(11)

    def swap(n):
        return beside(xs.at[n], xr.at[n], d_s.at[n], d_r.at[n])

    def chunk(n, dx):
        rows = pl.ds(pl.multiple_of(at_x(dx) * 192, 64), 192)
        gate = dot(nbuf[rows, :], wbuf[0:FFD, :], 1, 1)
        upward = dot(nbuf[rows, :], wbuf[FFD : 2 * FFD, :], 1, 1)
        hidden = (gate / (1.0 + jnp.exp(-gate)) * upward).astype(BF16)
        part = dot(hidden, wbuf[2 * FFD : 3 * FFD, :]).astype(BF16)

        @pl.when(core == 0)
        def _():
            po[n] = part[0:96]
            xs[n] = part[96:192]

        @pl.when(core == 1)
        def _():
            po[n] = part[96:192]
            xs[n] = part[0:96]

        swap(n).start()

    def hop(src, dst, to, k):
        return pltpu.make_async_remote_copy(
            src_ref=src, dst_ref=dst, send_sem=f_s.at[k], recv_sem=f_r.at[k],
            device_id=to_x(to, 0), device_id_type=mesh_id,
        )

    def summed(n):
        swap(n).wait_recv()
        return po[n].astype(F32) + xr[n].astype(F32)

    chunk(0, 2)
    chunk(1, 1)
    st[0] = summed(0).astype(BF16)
    hops = [
        hop(st.at[0, pl.ds(0, 48)], ra, 1, 0),
        hop(st.at[0, pl.ds(48, 48)], rb, -1, 1),
        hop(st.at[1, pl.ds(48, 48)], fa.at[pl.ds(48, 48)], 1, 2),
        hop(st.at[2, pl.ds(0, 48)], fb.at[pl.ds(0, 48)], -1, 3),
        hop(so.at[0], fa.at[pl.ds(0, 48)], 1, 4),
        hop(so.at[1], fb.at[pl.ds(48, 48)], -1, 5),
    ]
    hops[0].start()
    hops[1].start()
    chunk(2, 3)
    ahead = summed(1)
    st[1, 48:96, :] = ahead[48:96].astype(BF16)
    hops[2].start()
    chunk(3, 0)
    behind = summed(2)
    st[2, 0:48, :] = behind[0:48].astype(BF16)
    hops[3].start()
    hops[0].wait_recv()
    so[0] = (po[1, 0:48, :].astype(F32) + xr[1, 0:48, :].astype(F32) + ra[...].astype(F32)).astype(BF16)
    hops[4].start()
    hops[1].wait_recv()
    so[1] = (behind[48:96] + rb[...].astype(F32)).astype(BF16)
    hops[5].start()
    total = summed(3) + mid[pl.ds(pl.multiple_of(tp * OWN, 32), OWN), :].astype(F32)
    for h in hops[2:]:
        h.wait_recv()
    out_ref[...] = (total + fa[...].astype(F32) + fb[...].astype(F32)).astype(BF16)

    for flow in (lat, w_a, w_b, att):
        flow.finish()
    for rel in others:
        for far in (0, 1):
            share_lat(rel, far).wait_send()
        for dx in (1, -1):
            cross(rel, dx).wait_send()
    for dx in (0, -1, 1, 2):
        share_att(dx).wait_send()
    for n in range(4):
        swap(n).wait_send()
    for h in hops:
        h.wait_send()


def on_device(
    resid, query_small, query_large, kv_latent, rope_key, kv_gain, up_key_small, up_value_small,
    up_key_large, up_value_large, out_weight, mix_gain, gate_weight, up_weight, down_weight,
):
    rows = kv_latent.shape[0]
    positions = lax.axis_index("sp") * rows + jnp.arange(rows, dtype=jnp.int32)
    inverse = THETA ** (-jnp.arange(0, ROTARY, 2).astype(F32) / ROTARY)
    phase = inverse[:, None] * positions.astype(F32)[None, :]
    trig = jnp.concatenate([jnp.cos(phase), jnp.sin(phase)], axis=0)
    gains = jnp.concatenate([kv_gain, mix_gain]).reshape(1, 256 + D)

    vmem = pl.BlockSpec(memory_space=pltpu.VMEM)
    hbm = pl.BlockSpec(memory_space=pl.ANY)
    dma = pltpu.SemaphoreType.DMA
    return pl.pallas_call(
        kernel,
        out_shape=jax.ShapeDtypeStruct((OWN, D), BF16),
        in_specs=[vmem] * 10 + [hbm] * 5,
        out_specs=vmem,
        scratch_shapes=[
            pltpu.VMEM((16, LAT_ROWS, 256), BF16),
            pltpu.VMEM((3 * FFD, D), BF16),
            pltpu.VMEM((1536, D), BF16),
            pltpu.VMEM((ROWS, D), BF16),
            pltpu.VMEM((ROWS, D), BF16),
            pltpu.VMEM((8, 1152, 128), BF16),
            pltpu.VMEM((ROWS, 1536), BF16),
            pltpu.VMEM((96, ROWS), BF16),
            pltpu.VMEM((160, ROWS), BF16),
            pltpu.VMEM((256, 192), BF16),
            pltpu.VMEM((192, 256), BF16),
            pltpu.VMEM((ROWS, 96), BF16),
            pltpu.VMEM((ROWS, 160), BF16),
            pltpu.VMEM((80, ROWS), BF16),
            pltpu.VMEM((144, ROWS), BF16),
            pltpu.VMEM((1, ROWS), F32),
            pltpu.VMEM((1, ROWS), F32),
            pltpu.VMEM((80, ROWS), F32),
            pltpu.VMEM((144, ROWS), F32),
            pltpu.VMEM((4, OWN, D), BF16),
            pltpu.VMEM((4, OWN, D), BF16),
            pltpu.VMEM((4, OWN, D), BF16),
            pltpu.VMEM((48, D), BF16),
            pltpu.VMEM((48, D), BF16),
            pltpu.VMEM((OWN, D), BF16),
            pltpu.VMEM((OWN, D), BF16),
            pltpu.VMEM((3, OWN, D), BF16),
            pltpu.VMEM((2, 48, D), BF16),
            dma((5,)),
            *[dma((20,)) for _ in range(6)],
            *[dma((2, 16)) for _ in range(4)],
            *[dma((4,)) for _ in range(8)],
            dma((4,)), dma((4,)), dma((6,)), dma((6,)),
        ],
        compiler_params=pltpu.CompilerParams(
            collective_id=0, has_side_effects=True, vmem_limit_bytes=67043328
        ),
    )(
        kv_latent, rope_key.T, trig, gains, query_small.T, query_large.T,
        up_key_small.T, up_key_large, up_value_small.T, up_value_large,
        out_weight, resid, gate_weight.T, up_weight.T, down_weight.T,
    )


def solution(mesh):
    placed = (
        P(("sp", "tp"), None), P("sp", "tp"), P("sp", "tp"), P("sp", None), P("sp", None), P(),
        P(None, "tp"), P(None, "tp"), P(None, "tp"), P(None, "tp"), P(), P(),
        P("sp", "tp"), P("sp", "tp"), P("sp", "tp"),
    )
    return jax.shard_map(
        on_device, mesh=mesh, in_specs=placed, out_specs=P(("sp", "tp"), None), check_vma=False
    )
```

```python
import functools
import math

import jax
import jax.numpy as jnp
from jax import lax
from jax.experimental import pallas as pl
from jax.experimental.pallas import tpu as pltpu
from jax.sharding import PartitionSpec as P

NOPE_SMALL = 64
NOPE_LARGE = 128
ROTARY = 32
THETA = 10000.0
EPSILON = 1e-06
FLOOR = -1e30
ROWS = 768
LAT_ROWS = 896
D = 2048
OWN = 96
FFD = 704
QT = 256
MT = 256
F32 = jnp.float32
BF16 = jnp.bfloat16


def dot(a, b, ca=1, cb=0):
    return lax.dot_general(a, b, (((ca,), (cb,)), ((), ())), preferred_element_type=F32)


class Flow:
    def __init__(self, view, size, send_sem, recv_sem, block, target):
        self.view, self.size = view, size
        self.send_sem, self.recv_sem = send_sem, recv_sem
        self.block, self.target = block, target
        self.sent = []

    def copy(self, at, lo, size, to, k):
        ref = self.view(self.block(*at), lo, size)
        return pltpu.make_async_remote_copy(
            src_ref=ref,
            dst_ref=ref,
            send_sem=self.send_sem.at[k],
            recv_sem=self.recv_sem.at[k],
            device_id=self.target(*to),
            device_id_type=pl.DeviceIdType.MESH,
        )

    def send(self, at, part, to, k):
        lo, size = self.span(part)
        self.sent.append((at, lo, size, to, k))
        self.copy(at, lo, size, to, k).start()

    def span(self, part):
        half = self.size // 2
        return {None: (0, self.size), 0: (0, half), 1: (half, half)}[part]

    def wait(self, at, part, k):
        lo, size = self.span(part)
        self.copy(at, lo, size, (1, 0), k).wait_recv()

    def finish(self):
        for at, lo, size, to, k in self.sent:
            self.copy(at, lo, size, to, k).wait_send()

    def start_u(self):
        self.send((0, 0), None, (1, 0), 0)
        self.send((0, 0), None, (-1, 0), 1)

    def spread(self, du, k):
        self.send((du, 0), None, (0, 1), k)
        self.send((du, 0), None, (0, -1), k + 1)

    def relay_v(self, du, k):
        self.wait((du, -1), None, k)
        self.send((du, -1), 0, (0, 1), k + 2)
        self.wait((du, 1), None, k + 1)
        self.send((du, 1), 1, (0, -1), k + 3)

    def end_v(self, du, k):
        self.wait((du, 2), 0, k + 2)
        self.wait((du, 2), 1, k + 3)

    def event(self, n):
        if n == 0:
            self.start_u()
            self.spread(0, 4)
        elif n == 1:
            self.wait((-1, 0), None, 0)
            self.send((-1, 0), 0, (1, 0), 2)
            self.spread(-1, 8)
        elif n == 2:
            self.wait((1, 0), None, 1)
            self.send((1, 0), 1, (-1, 0), 3)
            self.spread(1, 12)
        elif n == 3:
            self.relay_v(0, 4)
        elif n == 4:
            self.wait((2, 0), 0, 2)
            self.wait((2, 0), 1, 3)
            self.spread(2, 16)
        elif n == 5:
            self.relay_v(-1, 8)
        elif n == 6:
            self.relay_v(1, 12)
        elif n == 7:
            self.relay_v(2, 16)
        else:
            du = (0, -1, 1, 2)[n - 8]
            self.end_v(du, 4 + 4 * (n - 8))

    def line(self, n):
        if n == 0:
            self.start_u()
        elif n == 1:
            self.wait((-1, 0), None, 0)
            self.send((-1, 0), 0, (1, 0), 2)
        elif n == 2:
            self.wait((1, 0), None, 1)
            self.send((1, 0), 1, (-1, 0), 3)
        elif n == 3:
            self.wait((2, 0), 0, 2)
            self.wait((2, 0), 1, 3)


def done_at(du, dv):
    if dv == 0:
        return {0: 0, -1: 1, 1: 2, 2: 4}[du]
    if dv == 2:
        return 8 + (0, -1, 1, 2).index(du)
    return {0: 3, -1: 5, 1: 6, 2: 7}[du]


def kernel(
    lat_ref, rk_ref, trig_ref, gain_ref, qs_in, ql_in, wks_ref, wkl_ref, wvs_ref, wvl_ref,
    ow_hbm, res_hbm, gate_hbm, up_hbm, down_hbm,
    out_ref,
    lbuf, wbuf, owbuf, mid, nbuf, obuf, abuf, qs_ref, ql_ref, wk_ref, wv_ref, ks, kl, vs, vl,
    ms, ml, acs, acl, po, xs, xr, ra, rb, fa, fb, st, so,
    cp, la_s, la_r, wa_s, wa_r, wb_s, wb_r, lb_s, lb_r, ls_s, ls_r,
    r_s, r_r, rs_s, rs_r, o_s, o_r, os_s, os_r, d_s, d_r, f_s, f_r,
):
    sp, tp = lax.axis_index("sp"), lax.axis_index("tp")
    z, y = sp // 4, lax.rem(sp, 4)
    x, core = tp // 2, lax.rem(tp, 2)
    mesh_id = pl.DeviceIdType.MESH

    def at_sp(dy, dz):
        return lax.rem(z + dz + 4, 4) * 4 + lax.rem(y + dy + 4, 4)

    def at_x(dx, _=0):
        return lax.rem(x + dx + 4, 4)

    sibling = {"tp": x * 2 + 1 - core}
    near = [{"sp": at_sp(*d)} for d in ((1, 0), (-1, 0), (0, 1), (0, -1))]
    near += [{"tp": at_x(d) * 2 + core} for d in (1, -1)] + [sibling]

    column = pl.ds(pl.multiple_of(sp * 128, 128), 128)
    local = [
        pltpu.make_async_copy(res_hbm, mid.at[pl.ds(pl.multiple_of(tp * OWN, 32), OWN)], cp.at[0]),
        pltpu.make_async_copy(gate_hbm, wbuf.at[0:FFD, column], cp.at[1]),
        pltpu.make_async_copy(up_hbm, wbuf.at[FFD : 2 * FFD, column], cp.at[2]),
        pltpu.make_async_copy(down_hbm, wbuf.at[2 * FFD : 3 * FFD, column], cp.at[3]),
        pltpu.make_async_copy(ow_hbm, owbuf, cp.at[4]),
    ]
    for c in local:
        c.start()
    barrier = pltpu.get_barrier_semaphore()
    for n in near:
        pl.semaphore_signal(barrier, inc=1, device_id=n, device_id_type=mesh_id)

    trig_cos, trig_sin = trig_ref[0:16, :], trig_ref[16:32, :]

    def turn(first, second):
        first, second = first.astype(F32), second.astype(F32)
        return (
            (first * trig_cos - second * trig_sin).astype(BF16),
            (second * trig_cos + first * trig_sin).astype(BF16),
        )

    wide = lat_ref[...].astype(F32)
    scaled = wide * lax.rsqrt(jnp.mean(wide * wide, axis=-1, keepdims=True) + EPSILON)
    lbuf[sp, 0:ROWS, :] = (scaled * gain_ref[:, 0:256].astype(F32)).astype(BF16)
    one, two = turn(rk_ref[0:16, :], rk_ref[16:32, :])
    for n in range(3):
        lbuf[sp, ROWS + 32 * n : ROWS + 32 * n + 16, :] = one[:, 256 * n : 256 * n + 256]
        lbuf[sp, ROWS + 32 * n + 16 : ROWS + 32 * n + 32, :] = two[:, 256 * n : 256 * n + 256]
    lbuf[sp, ROWS + 96 : LAT_ROWS, :] = jnp.zeros((LAT_ROWS - ROWS - 96, 256), BF16)
    pl.semaphore_wait(barrier, len(near))

    q_rows = LAT_ROWS // 4

    def lat_ref_of(block, far, c, lo=0, size=q_rows):
        base = (2 * lax.rem(x + far, 2) + c) * q_rows + lo
        return lbuf.at[block, pl.ds(pl.multiple_of(base, 16), size)]

    def lat_view(block, lo, size):
        return lat_ref_of(block, 0, core, lo, size)

    def w_view(piece):
        def view(block, lo, size):
            return wbuf.at[
                pl.ds(1056 * piece + lo, size), pl.ds(pl.multiple_of(block * 128, 128), 128)
            ]
        return view

    def yz(du, dv):
        return at_sp(du, dv)

    def zy(du, dv):
        return at_sp(dv, du)

    def to_yz(du, dv):
        return {"sp": at_sp(du, dv)}

    def to_zy(du, dv):
        return {"sp": at_sp(dv, du)}

    def to_x(du, _):
        return {"tp": at_x(du) * 2 + core}

    def by_core(du, dv):
        return at_sp(jnp.where(core == 0, du, dv), jnp.where(core == 0, dv, du))

    lat = Flow(lat_view, q_rows, la_s, la_r, by_core, lambda du, dv: {"sp": by_core(du, dv)})
    w_a = Flow(w_view(0), 1056, wa_s, wa_r, yz, to_yz)
    w_b = Flow(w_view(1), 1056, wb_s, wb_r, zy, to_zy)

    def res_view(chip, lo, size, c=None):
        c = core if c is None else c
        return mid.at[pl.ds(pl.multiple_of((chip * 2 + c) * OWN, 32) + lo, size)]

    def o_view(chip, lo, size, c=None):
        c = core if c is None else c
        return obuf.at[chip * 2 + c, pl.ds(lo, size)]

    res = Flow(res_view, OWN, r_s, r_r, at_x, to_x)
    att = Flow(o_view, 1152, o_s, o_r, at_x, to_x)

    def beside(src, dst, s, r):
        return pltpu.make_async_remote_copy(
            src_ref=src, dst_ref=dst, send_sem=s, recv_sem=r, device_id=sibling, device_id_type=mesh_id
        )

    def number(du, dv):
        return (dv % 4) * 4 + du % 4

    def number_by_core(du, dv):
        return jnp.where(core == 0, number(du, dv), number(dv, du))

    def share_lat(rel, far):
        ref = lat_ref_of(by_core(*rel), far, core)
        n = number_by_core(*rel)
        return beside(ref, ref, ls_s.at[far, n], ls_r.at[far, n])

    def shared_lat(rel, far):
        ref = lat_ref_of(at_sp(*rel), far, 1 - core)
        n = number(*rel)
        return beside(ref, ref, ls_s.at[far, n], ls_r.at[far, n])

    def cross(rel, dx, far=0):
        half = 0 if dx == 1 else 1
        ref = lat_ref_of(by_core(*rel), far, core, half * (q_rows // 2), q_rows // 2)
        n = number(*rel)
        return pltpu.make_async_remote_copy(
            src_ref=ref, dst_ref=ref, send_sem=lb_s.at[half, n], recv_sem=lb_r.at[half, n],
            device_id=to_x(dx, 0), device_id_type=mesh_id,
        )

    def share_line(view, size, s, r, dx, c=None):
        ref = view(at_x(dx), 0, size, c)
        return beside(ref, ref, s.at[dx % 4], r.at[dx % 4])

    share_res = functools.partial(share_line, res_view, OWN, rs_s, rs_r)
    share_att = functools.partial(share_line, o_view, 1152, os_s, os_r)

    others = [
        (-1, 0), (1, 0), (0, -1), (0, 1), (-1, -1), (-1, 1), (1, -1), (1, 1),
        (2, 0), (0, 2), (2, -1), (-1, 2), (2, 1), (1, 2), (2, 2),
    ]

    def lat_event(n):
        lat.event(n)
        for rel in others:
            if done_at(*rel) == n:
                cross(rel, 1).start()
                cross(rel, -1).start()
                share_lat(rel, 0).start()

    def lat_crossed(rel):
        cross(rel, 1, 1).wait_recv()
        cross(rel, -1, 1).wait_recv()
        share_lat(rel, 1).start()

    scale_small = math.log2(math.e) / math.sqrt(NOPE_SMALL + ROTARY)
    scale_large = math.log2(math.e) / math.sqrt(NOPE_LARGE + ROTARY)

    def expand(block):
        latent = lbuf[block, 0:ROWS, :]
        keys = dot(latent, wk_ref[...]).astype(BF16)
        kl[:, 0:128] = keys[:, 0:128]
        ks[:, 0:64] = keys[:, 128:192]
        for n in range(3):
            turned = lbuf[block, ROWS + 32 * n : ROWS + 32 * n + 32, :]
            turned = turned.astype(F32).T.astype(BF16)
            ks[256 * n : 256 * n + 256, 64:96] = turned
            kl[256 * n : 256 * n + 256, 128:160] = turned
        values = dot(wv_ref[...], latent, 1, 1).astype(BF16)
        vl[0:128, :] = values[0:128]
        vs[0:64, :] = values[128:192]

    heads = (
        (ql_ref, kl, vl, ml, acl, scale_large),
        (qs_ref, ks, vs, ms, acs, scale_small),
    )

    def attend(block, diagonal):
        expand(block)
        units = [(i, h) for i in range(ROWS // QT) for h in heads]
        scores, soft = {}, {}

        def score(u):
            i, (q, k, *_) = units[u]
            scores[u] = dot(k[...], q[:, i * QT : i * QT + QT])

        def weigh(u):
            i, (_, _, _, m, _, scale) = units[u]
            s, cols = scores.pop(u), slice(i * QT, i * QT + QT)
            if diagonal:
                row = lax.broadcasted_iota(jnp.int32, (ROWS, QT), 0)
                col = lax.broadcasted_iota(jnp.int32, (ROWS, QT), 1) + i * QT
                s = jnp.where(row <= col, s, FLOOR)
                new = jnp.max(s, axis=0, keepdims=True)
                fade = None
            else:
                old = m[:, cols]
                new = jnp.maximum(old, jnp.max(s, axis=0, keepdims=True))
                fade = jnp.exp2((old - new) * scale)
            m[:, cols] = new
            soft[u] = (jnp.exp2((s - new) * scale).astype(BF16), fade)

        def gather(u):
            i, (_, _, v, _, acc, _) = units[u]
            (p, fade), cols = soft.pop(u), slice(i * QT, i * QT + QT)
            o = dot(v[...], p)
            acc[:, cols] = o if diagonal else acc[:, cols] * fade + o

        score(0)
        score(1)
        for u in range(len(units)):
            if u + 2 < len(units):
                score(u + 2)
            weigh(u)
            if u > 0:
                gather(u - 1)
        gather(len(units) - 1)

    lat_event(0)
    local[0].wait()

    for inp, ref, nope in ((qs_in, qs_ref, NOPE_SMALL), (ql_in, ql_ref, NOPE_LARGE)):
        ref[0:nope, :] = inp[0:nope, :]
        one, two = turn(inp[nope : nope + 16, :], inp[nope + 16 : nope + 32, :])
        ref[nope : nope + 16, :] = one
        ref[nope + 16 : nope + 32, :] = two
    wk_ref[:, 0:128] = wkl_ref[...]
    wk_ref[:, 128:192] = wks_ref[...].astype(F32).T.astype(BF16)
    wv_ref[0:128, :] = wvl_ref[...].astype(F32).T.astype(BF16)
    wv_ref[128:192, :] = wvs_ref[...]
    vs[64:80, :] = jnp.ones((16, ROWS), BF16)
    vl[128:144, :] = jnp.ones((16, ROWS), BF16)

    attend(sp, True)
    for n in range(1, 4):
        lat_event(n)
    for c in local[1:4]:
        c.wait()

    def w_event(n):
        w_a.event(n)
        w_b.event(n)

    def w_first(n):
        for w in (w_a, w_b):
            w.start_u() if n == 0 else w.spread(0, 4)

    def res_event(n):
        res.line(n)
        share_res((0, -1, 1, 2)[n]).start()

    order = sorted(others, key=lambda rel: done_at(*rel))
    todo = {t: [] for t in range(1, 16)}
    todo[1] += [(lat_event, 4), (w_first, 0)]
    todo[1] += [(lat_crossed, order[n]) for n in range(4)]
    todo[2] += [(lat_event, 5), (lat_event, 6), (lat_crossed, order[4])]
    todo[3] += [(lat_event, 7), (lat_event, 8), (w_first, 1), (lat_crossed, order[5]), (lat_crossed, order[6])]
    todo[4] += [(lat_event, 9), (lat_event, 10), (lat_event, 11), (lat_crossed, order[7]), (lat_crossed, order[8])]
    todo[5] += [(lat_crossed, order[9]), (lat_crossed, order[10])]
    todo[6] += [(lat_crossed, order[11]), (lat_crossed, order[12]), (res_event, 0)]
    todo[7] += [(lat_crossed, order[13]), (lat_crossed, order[14])]
    for t, n in ((14, 1), (15, 2)):
        todo[t].append((res_event, n))
    for t, n in ((8, 1), (9, 2), (10, 3)):
        todo[t].append((w_event, n))
    for t, rel in enumerate(others):
        todo[t + 1].append((lambda r: shared_lat(r, 0).wait_recv(), rel))
        todo[t + 1].append((lambda r: shared_lat(r, 1).wait_recv(), rel))

    def step(t, carry):
        dy, dz = 0, 0
        for n in range(1, 16):
            dy = jnp.where(t == n, others[n - 1][0], dy)
            dz = jnp.where(t == n, others[n - 1][1], dz)

            @pl.when(t == n)
            def _():
                for what, arg in todo[n]:
                    what(arg)
        block = at_sp(dy, dz)

        @pl.when(block < sp)
        def _():
            attend(block, False)
        return carry

    lax.fori_loop(1, 16, step, 0)

    mine = obuf.at[tp]
    mine[0:ROWS, :] = (acl[0:128, :] / acl[128:129, :]).T.astype(BF16)
    small = acs[0:64, :] / acs[64:65, :]
    small = jnp.concatenate([small[:, 0:384], small[:, 384:768]], axis=0)
    mine[ROWS:1152, :] = small.T.astype(BF16)
    left = lax.broadcasted_iota(jnp.int32, (384, 128), 1) < 64
    att.line(0)
    share_att(0).start()
    w_event(4)
    for n in range(1, 4):
        att.line(n)
        share_att((-1, 1, 2)[n - 1]).start()
        w_event(4 + n)
    res_event(3)
    for dx in (0, -1, 1, 2):
        share_att(dx, 1 - core).wait_recv()
        share_res(dx, 1 - core).wait_recv()
    for n in range(8):
        abuf[:, 512 + 128 * n : 640 + 128 * n] = obuf[n, 0:ROWS, :]
    for n in range(4):
        one = obuf[2 * n, ROWS:1152, :].astype(F32)
        two = obuf[2 * n + 1, ROWS:1152, :].astype(F32)
        abuf[0:384, 128 * n : 128 * n + 128] = jnp.where(left, one, pltpu.roll(two, 64, 1)).astype(BF16)
        abuf[384:768, 128 * n : 128 * n + 128] = jnp.where(left, pltpu.roll(one, 64, 1), two).astype(BF16)
    local[4].wait()
    res.finish()
    for dx in (0, -1, 1, 2):
        share_res(dx).wait_send()

    def project(i, carry):
        for n in range(3):
            @pl.when(i == n)
            def _():
                w_event(8 + n)
        rows = pl.ds(pl.multiple_of(i * MT, MT), MT)
        wide = dot(abuf[rows, :], owbuf[...]) + mid[rows, :].astype(F32)
        middle = wide.astype(BF16)
        mid[rows, :] = middle
        wide = middle.astype(F32)
        scaled = wide * lax.rsqrt(jnp.mean(wide * wide, axis=-1, keepdims=True) + EPSILON)
        nbuf[rows, :] = (scaled * gain_ref[:, 256:].astype(F32)).astype(BF16)
        return carry

    lax.fori_loop(0, ROWS // MT, project, 0)
    w_event(11)

    def swap(n):
        return beside(xs.at[n], xr.at[n], d_s.at[n], d_r.at[n])

    def chunk(n, dx):
        rows = pl.ds(pl.multiple_of(at_x(dx) * 192, 64), 192)
        gate = dot(nbuf[rows, :], wbuf[0:FFD, :], 1, 1)
        upward = dot(nbuf[rows, :], wbuf[FFD : 2 * FFD, :], 1, 1)
        hidden = (gate / (1.0 + jnp.exp(-gate)) * upward).astype(BF16)
        part = dot(hidden, wbuf[2 * FFD : 3 * FFD, :]).astype(BF16)

        @pl.when(core == 0)
        def _():
            po[n] = part[0:96]
            xs[n] = part[96:192]

        @pl.when(core == 1)
        def _():
            po[n] = part[96:192]
            xs[n] = part[0:96]

        swap(n).start()

    def hop(src, dst, to, k):
        return pltpu.make_async_remote_copy(
            src_ref=src, dst_ref=dst, send_sem=f_s.at[k], recv_sem=f_r.at[k],
            device_id=to_x(to, 0), device_id_type=mesh_id,
        )

    def summed(n):
        swap(n).wait_recv()
        return po[n].astype(F32) + xr[n].astype(F32)

    chunk(0, 2)
    chunk(1, 1)
    st[0] = summed(0).astype(BF16)
    hops = [
        hop(st.at[0, pl.ds(0, 48)], ra, 1, 0),
        hop(st.at[0, pl.ds(48, 48)], rb, -1, 1),
        hop(st.at[1, pl.ds(48, 48)], fa.at[pl.ds(48, 48)], 1, 2),
        hop(st.at[2, pl.ds(0, 48)], fb.at[pl.ds(0, 48)], -1, 3),
        hop(so.at[0], fa.at[pl.ds(0, 48)], 1, 4),
        hop(so.at[1], fb.at[pl.ds(48, 48)], -1, 5),
    ]
    hops[0].start()
    hops[1].start()
    chunk(2, 3)
    ahead = summed(1)
    st[1, 48:96, :] = ahead[48:96].astype(BF16)
    hops[2].start()
    chunk(3, 0)
    behind = summed(2)
    st[2, 0:48, :] = behind[0:48].astype(BF16)
    hops[3].start()
    hops[0].wait_recv()
    so[0] = (po[1, 0:48, :].astype(F32) + xr[1, 0:48, :].astype(F32) + ra[...].astype(F32)).astype(BF16)
    hops[4].start()
    hops[1].wait_recv()
    so[1] = (behind[48:96] + rb[...].astype(F32)).astype(BF16)
    hops[5].start()
    total = summed(3) + mid[pl.ds(pl.multiple_of(tp * OWN, 32), OWN), :].astype(F32)
    for h in hops[2:]:
        h.wait_recv()
    out_ref[...] = (total + fa[...].astype(F32) + fb[...].astype(F32)).astype(BF16)

    for flow in (lat, w_a, w_b, att):
        flow.finish()
    for rel in others:
        for far in (0, 1):
            share_lat(rel, far).wait_send()
        for dx in (1, -1):
            cross(rel, dx).wait_send()
    for dx in (0, -1, 1, 2):
        share_att(dx).wait_send()
    for n in range(4):
        swap(n).wait_send()
    for h in hops:
        h.wait_send()


def on_device(
    resid, query_small, query_large, kv_latent, rope_key, kv_gain, up_key_small, up_value_small,
    up_key_large, up_value_large, out_weight, mix_gain, gate_weight, up_weight, down_weight,
):
    rows = kv_latent.shape[0]
    positions = lax.axis_index("sp") * rows + jnp.arange(rows, dtype=jnp.int32)
    inverse = THETA ** (-jnp.arange(0, ROTARY, 2).astype(F32) / ROTARY)
    phase = inverse[:, None] * positions.astype(F32)[None, :]
    trig = jnp.concatenate([jnp.cos(phase), jnp.sin(phase)], axis=0)
    gains = jnp.concatenate([kv_gain, mix_gain]).reshape(1, 256 + D)

    vmem = pl.BlockSpec(memory_space=pltpu.VMEM)
    hbm = pl.BlockSpec(memory_space=pl.ANY)
    dma = pltpu.SemaphoreType.DMA
    return pl.pallas_call(
        kernel,
        out_shape=jax.ShapeDtypeStruct((OWN, D), BF16),
        in_specs=[vmem] * 10 + [hbm] * 5,
        out_specs=vmem,
        scratch_shapes=[
            pltpu.VMEM((16, LAT_ROWS, 256), BF16),
            pltpu.VMEM((3 * FFD, D), BF16),
            pltpu.VMEM((1536, D), BF16),
            pltpu.VMEM((ROWS, D), BF16),
            pltpu.VMEM((ROWS, D), BF16),
            pltpu.VMEM((8, 1152, 128), BF16),
            pltpu.VMEM((ROWS, 1536), BF16),
            pltpu.VMEM((96, ROWS), BF16),
            pltpu.VMEM((160, ROWS), BF16),
            pltpu.VMEM((256, 192), BF16),
            pltpu.VMEM((192, 256), BF16),
            pltpu.VMEM((ROWS, 96), BF16),
            pltpu.VMEM((ROWS, 160), BF16),
            pltpu.VMEM((80, ROWS), BF16),
            pltpu.VMEM((144, ROWS), BF16),
            pltpu.VMEM((1, ROWS), F32),
            pltpu.VMEM((1, ROWS), F32),
            pltpu.VMEM((80, ROWS), F32),
            pltpu.VMEM((144, ROWS), F32),
            pltpu.VMEM((4, OWN, D), BF16),
            pltpu.VMEM((4, OWN, D), BF16),
            pltpu.VMEM((4, OWN, D), BF16),
            pltpu.VMEM((48, D), BF16),
            pltpu.VMEM((48, D), BF16),
            pltpu.VMEM((OWN, D), BF16),
            pltpu.VMEM((OWN, D), BF16),
            pltpu.VMEM((3, OWN, D), BF16),
            pltpu.VMEM((2, 48, D), BF16),
            dma((5,)),
            *[dma((20,)) for _ in range(6)],
            *[dma((2, 16)) for _ in range(4)],
            *[dma((4,)) for _ in range(8)],
            dma((4,)), dma((4,)), dma((6,)), dma((6,)),
        ],
        compiler_params=pltpu.CompilerParams(
            collective_id=0, has_side_effects=True, vmem_limit_bytes=67043328
        ),
    )(
        kv_latent, rope_key.T, trig, gains, query_small.T, query_large.T,
        up_key_small.T, up_key_large, up_value_small.T, up_value_large,
        out_weight, resid, gate_weight.T, up_weight.T, down_weight.T,
    )


def solution(mesh):
    placed = (
        P(("sp", "tp"), None), P("sp", "tp"), P("sp", "tp"), P("sp", None), P("sp", None), P(),
        P(None, "tp"), P(None, "tp"), P(None, "tp"), P(None, "tp"), P(), P(),
        P("sp", "tp"), P("sp", "tp"), P("sp", "tp"),
    )
    return jax.shard_map(
        on_device, mesh=mesh, in_specs=placed, out_specs=P(("sp", "tp"), None), check_vma=False
    )
```

```python
import functools
import math

import jax
import jax.numpy as jnp
from jax import lax
from jax.experimental import pallas as pl
from jax.experimental.pallas import tpu as pltpu
from jax.sharding import PartitionSpec as P

NOPE_SMALL = 64
NOPE_LARGE = 128
ROTARY = 32
THETA = 10000.0
EPSILON = 1e-06
FLOOR = -1e30
ROWS = 768
LAT_ROWS = 896
D = 2048
OWN = 96
FFD = 704
QT = 256
MT = 256
F32 = jnp.float32
BF16 = jnp.bfloat16


def dot(a, b, ca=1, cb=0):
    return lax.dot_general(a, b, (((ca,), (cb,)), ((), ())), preferred_element_type=F32)


class Flow:
    def __init__(self, view, size, send_sem, recv_sem, block, target):
        self.view, self.size = view, size
        self.send_sem, self.recv_sem = send_sem, recv_sem
        self.block, self.target = block, target
        self.sent = []

    def copy(self, at, lo, size, to, k):
        ref = self.view(self.block(*at), lo, size)
        return pltpu.make_async_remote_copy(
            src_ref=ref,
            dst_ref=ref,
            send_sem=self.send_sem.at[k],
            recv_sem=self.recv_sem.at[k],
            device_id=self.target(*to),
            device_id_type=pl.DeviceIdType.MESH,
        )

    def send(self, at, part, to, k):
        lo, size = self.span(part)
        self.sent.append((at, lo, size, to, k))
        self.copy(at, lo, size, to, k).start()

    def span(self, part):
        half = self.size // 2
        return {None: (0, self.size), 0: (0, half), 1: (half, half)}[part]

    def wait(self, at, part, k):
        lo, size = self.span(part)
        self.copy(at, lo, size, (1, 0), k).wait_recv()

    def finish(self):
        for at, lo, size, to, k in self.sent:
            self.copy(at, lo, size, to, k).wait_send()

    def start_u(self):
        self.send((0, 0), None, (1, 0), 0)
        self.send((0, 0), None, (-1, 0), 1)

    def spread(self, du, k):
        self.send((du, 0), None, (0, 1), k)
        self.send((du, 0), None, (0, -1), k + 1)

    def relay_v(self, du, k):
        self.wait((du, -1), None, k)
        self.send((du, -1), 0, (0, 1), k + 2)
        self.wait((du, 1), None, k + 1)
        self.send((du, 1), 1, (0, -1), k + 3)

    def end_v(self, du, k):
        self.wait((du, 2), 0, k + 2)
        self.wait((du, 2), 1, k + 3)

    def event(self, n):
        if n == 0:
            self.start_u()
            self.spread(0, 4)
        elif n == 1:
            self.wait((-1, 0), None, 0)
            self.send((-1, 0), 0, (1, 0), 2)
            self.spread(-1, 8)
        elif n == 2:
            self.wait((1, 0), None, 1)
            self.send((1, 0), 1, (-1, 0), 3)
            self.spread(1, 12)
        elif n == 3:
            self.relay_v(0, 4)
        elif n == 4:
            self.wait((2, 0), 0, 2)
            self.wait((2, 0), 1, 3)
            self.spread(2, 16)
        elif n == 5:
            self.relay_v(-1, 8)
        elif n == 6:
            self.relay_v(1, 12)
        elif n == 7:
            self.relay_v(2, 16)
        else:
            du = (0, -1, 1, 2)[n - 8]
            self.end_v(du, 4 + 4 * (n - 8))

    def line(self, n):
        if n == 0:
            self.start_u()
        elif n == 1:
            self.wait((-1, 0), None, 0)
            self.send((-1, 0), 0, (1, 0), 2)
        elif n == 2:
            self.wait((1, 0), None, 1)
            self.send((1, 0), 1, (-1, 0), 3)
        elif n == 3:
            self.wait((2, 0), 0, 2)
            self.wait((2, 0), 1, 3)


def done_at(du, dv):
    if dv == 0:
        return {0: 0, -1: 1, 1: 2, 2: 4}[du]
    if dv == 2:
        return 8 + (0, -1, 1, 2).index(du)
    return {0: 3, -1: 5, 1: 6, 2: 7}[du]


def kernel(
    lat_ref, rk_ref, trig_ref, gain_ref, qs_in, ql_in, wks_ref, wkl_ref, wvs_ref, wvl_ref,
    ow_hbm, res_hbm, gate_hbm, up_hbm, down_hbm,
    out_ref,
    lbuf, wbuf, owbuf, mid, nbuf, obuf, abuf, qs_ref, ql_ref, wk_ref, wv_ref, ks, kl, vs, vl,
    ms, ml, acs, acl, po, xs, xr, ra, rb, fa, fb, st, so,
    cp, la_s, la_r, wa_s, wa_r, wb_s, wb_r, lb_s, lb_r, ls_s, ls_r,
    r_s, r_r, rs_s, rs_r, o_s, o_r, os_s, os_r, d_s, d_r, f_s, f_r,
):
    sp, tp = lax.axis_index("sp"), lax.axis_index("tp")
    z, y = sp // 4, lax.rem(sp, 4)
    x, core = tp // 2, lax.rem(tp, 2)
    mesh_id = pl.DeviceIdType.MESH

    def at_sp(dy, dz):
        return lax.rem(z + dz + 4, 4) * 4 + lax.rem(y + dy + 4, 4)

    def at_x(dx, _=0):
        return lax.rem(x + dx + 4, 4)

    sibling = {"tp": x * 2 + 1 - core}
    near = [{"sp": at_sp(*d)} for d in ((1, 0), (-1, 0), (0, 1), (0, -1))]
    near += [{"tp": at_x(d) * 2 + core} for d in (1, -1)] + [sibling]

    column = pl.ds(pl.multiple_of(sp * 128, 128), 128)
    local = [
        pltpu.make_async_copy(res_hbm, mid.at[pl.ds(pl.multiple_of(tp * OWN, 32), OWN)], cp.at[0]),
        pltpu.make_async_copy(gate_hbm, wbuf.at[0:FFD, column], cp.at[1]),
        pltpu.make_async_copy(up_hbm, wbuf.at[FFD : 2 * FFD, column], cp.at[2]),
        pltpu.make_async_copy(down_hbm, wbuf.at[2 * FFD : 3 * FFD, column], cp.at[3]),
        pltpu.make_async_copy(ow_hbm, owbuf, cp.at[4]),
    ]
    for c in local:
        c.start()
    barrier = pltpu.get_barrier_semaphore()
    for n in near:
        pl.semaphore_signal(barrier, inc=1, device_id=n, device_id_type=mesh_id)

    trig_cos, trig_sin = trig_ref[0:16, :], trig_ref[16:32, :]

    def turn(first, second):
        first, second = first.astype(F32), second.astype(F32)
        return (
            (first * trig_cos - second * trig_sin).astype(BF16),
            (second * trig_cos + first * trig_sin).astype(BF16),
        )

    wide = lat_ref[...].astype(F32)
    scaled = wide * lax.rsqrt(jnp.mean(wide * wide, axis=-1, keepdims=True) + EPSILON)
    lbuf[sp, 0:ROWS, :] = (scaled * gain_ref[:, 0:256].astype(F32)).astype(BF16)
    one, two = turn(rk_ref[0:16, :], rk_ref[16:32, :])
    for n in range(3):
        lbuf[sp, ROWS + 32 * n : ROWS + 32 * n + 16, :] = one[:, 256 * n : 256 * n + 256]
        lbuf[sp, ROWS + 32 * n + 16 : ROWS + 32 * n + 32, :] = two[:, 256 * n : 256 * n + 256]
    lbuf[sp, ROWS + 96 : LAT_ROWS, :] = jnp.zeros((LAT_ROWS - ROWS - 96, 256), BF16)
    pl.semaphore_wait(barrier, len(near))

    q_rows = LAT_ROWS // 4

    def lat_ref_of(block, far, c, lo=0, size=q_rows):
        base = (2 * lax.rem(x + far, 2) + c) * q_rows + lo
        return lbuf.at[block, pl.ds(pl.multiple_of(base, 16), size)]

    def lat_view(block, lo, size):
        return lat_ref_of(block, 0, core, lo, size)

    def w_view(piece):
        def view(block, lo, size):
            return wbuf.at[
                pl.ds(1056 * piece + lo, size), pl.ds(pl.multiple_of(block * 128, 128), 128)
            ]
        return view

    def yz(du, dv):
        return at_sp(du, dv)

    def zy(du, dv):
        return at_sp(dv, du)

    def to_yz(du, dv):
        return {"sp": at_sp(du, dv)}

    def to_zy(du, dv):
        return {"sp": at_sp(dv, du)}

    def to_x(du, _):
        return {"tp": at_x(du) * 2 + core}

    def by_core(du, dv):
        return at_sp(jnp.where(core == 0, du, dv), jnp.where(core == 0, dv, du))

    lat = Flow(lat_view, q_rows, la_s, la_r, by_core, lambda du, dv: {"sp": by_core(du, dv)})
    w_a = Flow(w_view(0), 1056, wa_s, wa_r, yz, to_yz)
    w_b = Flow(w_view(1), 1056, wb_s, wb_r, zy, to_zy)

    def res_view(chip, lo, size, c=None):
        c = core if c is None else c
        return mid.at[pl.ds(pl.multiple_of((chip * 2 + c) * OWN, 32) + lo, size)]

    def o_view(chip, lo, size, c=None):
        c = core if c is None else c
        return obuf.at[chip * 2 + c, pl.ds(lo, size)]

    res = Flow(res_view, OWN, r_s, r_r, at_x, to_x)
    att = Flow(o_view, 1152, o_s, o_r, at_x, to_x)

    def beside(src, dst, s, r):
        return pltpu.make_async_remote_copy(
            src_ref=src, dst_ref=dst, send_sem=s, recv_sem=r, device_id=sibling, device_id_type=mesh_id
        )

    def number(du, dv):
        return (dv % 4) * 4 + du % 4

    def number_by_core(du, dv):
        return jnp.where(core == 0, number(du, dv), number(dv, du))

    def share_lat(rel, far):
        ref = lat_ref_of(by_core(*rel), far, core)
        n = number_by_core(*rel)
        return beside(ref, ref, ls_s.at[far, n], ls_r.at[far, n])

    def shared_lat(rel, far):
        ref = lat_ref_of(at_sp(*rel), far, 1 - core)
        n = number(*rel)
        return beside(ref, ref, ls_s.at[far, n], ls_r.at[far, n])

    def cross(rel, dx, far=0):
        half = 0 if dx == 1 else 1
        ref = lat_ref_of(by_core(*rel), far, core, half * (q_rows // 2), q_rows // 2)
        n = number(*rel)
        return pltpu.make_async_remote_copy(
            src_ref=ref, dst_ref=ref, send_sem=lb_s.at[half, n], recv_sem=lb_r.at[half, n],
            device_id=to_x(dx, 0), device_id_type=mesh_id,
        )

    def share_line(view, size, s, r, dx, c=None):
        ref = view(at_x(dx), 0, size, c)
        return beside(ref, ref, s.at[dx % 4], r.at[dx % 4])

    share_res = functools.partial(share_line, res_view, OWN, rs_s, rs_r)
    share_att = functools.partial(share_line, o_view, 1152, os_s, os_r)

    others = [
        (-1, 0), (1, 0), (0, -1), (0, 1), (-1, -1), (-1, 1), (1, -1), (1, 1),
        (2, 0), (0, 2), (2, -1), (-1, 2), (2, 1), (1, 2), (2, 2),
    ]

    def lat_event(n):
        lat.event(n)
        for rel in others:
            if done_at(*rel) == n:
                cross(rel, 1).start()
                cross(rel, -1).start()
                share_lat(rel, 0).start()

    def lat_crossed(rel):
        cross(rel, 1, 1).wait_recv()
        cross(rel, -1, 1).wait_recv()
        share_lat(rel, 1).start()

    scale_small = math.log2(math.e) / math.sqrt(NOPE_SMALL + ROTARY)
    scale_large = math.log2(math.e) / math.sqrt(NOPE_LARGE + ROTARY)

    def expand(block):
        latent = lbuf[block, 0:ROWS, :]
        keys = dot(latent, wk_ref[...]).astype(BF16)
        kl[:, 0:128] = keys[:, 0:128]
        ks[:, 0:64] = keys[:, 128:192]
        for n in range(3):
            turned = lbuf[block, ROWS + 32 * n : ROWS + 32 * n + 32, :]
            turned = turned.astype(F32).T.astype(BF16)
            ks[256 * n : 256 * n + 256, 64:96] = turned
            kl[256 * n : 256 * n + 256, 128:160] = turned
        values = dot(wv_ref[...], latent, 1, 1).astype(BF16)
        vl[0:128, :] = values[0:128]
        vs[0:64, :] = values[128:192]

    heads = (
        (ql_ref, kl, vl, ml, acl, scale_large),
        (qs_ref, ks, vs, ms, acs, scale_small),
    )

    def attend(block, diagonal):
        expand(block)
        units = [(i, h) for i in range(ROWS // QT) for h in heads]
        scores, soft = {}, {}

        def score(u):
            i, (q, k, *_) = units[u]
            scores[u] = dot(k[...], q[:, i * QT : i * QT + QT])

        def weigh(u):
            i, (_, _, _, m, _, scale) = units[u]
            s, cols = scores.pop(u), slice(i * QT, i * QT + QT)
            if diagonal:
                row = lax.broadcasted_iota(jnp.int32, (ROWS, QT), 0)
                col = lax.broadcasted_iota(jnp.int32, (ROWS, QT), 1) + i * QT
                s = jnp.where(row <= col, s, FLOOR)
                new = jnp.max(s, axis=0, keepdims=True)
                fade = None
            else:
                old = m[:, cols]
                new = jnp.maximum(old, jnp.max(s, axis=0, keepdims=True))
                fade = jnp.exp2((old - new) * scale)
            m[:, cols] = new
            soft[u] = (jnp.exp2((s - new) * scale).astype(BF16), fade)

        def gather(u):
            i, (_, _, v, _, acc, _) = units[u]
            (p, fade), cols = soft.pop(u), slice(i * QT, i * QT + QT)
            o = dot(v[...], p)
            acc[:, cols] = o if diagonal else acc[:, cols] * fade + o

        score(0)
        score(1)
        for u in range(len(units)):
            if u + 2 < len(units):
                score(u + 2)
            weigh(u)
            if u > 0:
                gather(u - 1)
        gather(len(units) - 1)

    lat_event(0)
    local[0].wait()

    for inp, ref, nope in ((qs_in, qs_ref, NOPE_SMALL), (ql_in, ql_ref, NOPE_LARGE)):
        ref[0:nope, :] = inp[0:nope, :]
        one, two = turn(inp[nope : nope + 16, :], inp[nope + 16 : nope + 32, :])
        ref[nope : nope + 16, :] = one
        ref[nope + 16 : nope + 32, :] = two
    wk_ref[:, 0:128] = wkl_ref[...]
    wk_ref[:, 128:192] = wks_ref[...].astype(F32).T.astype(BF16)
    wv_ref[0:128, :] = wvl_ref[...].astype(F32).T.astype(BF16)
    wv_ref[128:192, :] = wvs_ref[...]
    vs[64:80, :] = jnp.ones((16, ROWS), BF16)
    vl[128:144, :] = jnp.ones((16, ROWS), BF16)

    attend(sp, True)
    for n in range(1, 4):
        lat_event(n)
    for c in local[1:4]:
        c.wait()

    def w_event(n):
        w_a.event(n)
        w_b.event(n)

    def w_first(n):
        for w in (w_a, w_b):
            w.start_u() if n == 0 else w.spread(0, 4)

    def res_event(n):
        res.line(n)
        share_res((0, -1, 1, 2)[n]).start()

    order = sorted(others, key=lambda rel: done_at(*rel))
    todo = {t: [] for t in range(1, 16)}
    todo[1] += [(lat_event, 4), (w_first, 0)]
    todo[1] += [(lat_crossed, order[n]) for n in range(4)]
    todo[2] += [(lat_event, 5), (lat_event, 6), (lat_crossed, order[4])]
    todo[3] += [(lat_event, 7), (lat_event, 8), (w_first, 1), (lat_crossed, order[5]), (lat_crossed, order[6])]
    todo[4] += [(lat_event, 9), (lat_event, 10), (lat_event, 11), (lat_crossed, order[7]), (lat_crossed, order[8])]
    todo[5] += [(lat_crossed, order[9]), (lat_crossed, order[10])]
    todo[6] += [(lat_crossed, order[11]), (lat_crossed, order[12]), (res_event, 0)]
    todo[7] += [(lat_crossed, order[13]), (lat_crossed, order[14])]
    for t, n in ((12, 1), (13, 2)):
        todo[t].append((res_event, n))
    for t, n in ((8, 1), (9, 2), (10, 3)):
        todo[t].append((w_event, n))
    for t, rel in enumerate(others):
        todo[t + 1].append((lambda r: shared_lat(r, 0).wait_recv(), rel))
        todo[t + 1].append((lambda r: shared_lat(r, 1).wait_recv(), rel))

    def step(t, carry):
        dy, dz = 0, 0
        for n in range(1, 16):
            dy = jnp.where(t == n, others[n - 1][0], dy)
            dz = jnp.where(t == n, others[n - 1][1], dz)

            @pl.when(t == n)
            def _():
                for what, arg in todo[n]:
                    what(arg)
        block = at_sp(dy, dz)

        @pl.when(block < sp)
        def _():
            attend(block, False)
        return carry

    lax.fori_loop(1, 16, step, 0)

    mine = obuf.at[tp]
    mine[0:ROWS, :] = (acl[0:128, :] / acl[128:129, :]).T.astype(BF16)
    small = acs[0:64, :] / acs[64:65, :]
    small = jnp.concatenate([small[:, 0:384], small[:, 384:768]], axis=0)
    mine[ROWS:1152, :] = small.T.astype(BF16)
    left = lax.broadcasted_iota(jnp.int32, (384, 128), 1) < 64
    att.line(0)
    share_att(0).start()
    w_event(4)
    for n in range(1, 4):
        att.line(n)
        share_att((-1, 1, 2)[n - 1]).start()
        w_event(4 + n)
    res_event(3)
    for dx in (0, -1, 1, 2):
        share_att(dx, 1 - core).wait_recv()
        share_res(dx, 1 - core).wait_recv()
    for n in range(8):
        abuf[:, 512 + 128 * n : 640 + 128 * n] = obuf[n, 0:ROWS, :]
    for n in range(4):
        one = obuf[2 * n, ROWS:1152, :].astype(F32)
        two = obuf[2 * n + 1, ROWS:1152, :].astype(F32)
        abuf[0:384, 128 * n : 128 * n + 128] = jnp.where(left, one, pltpu.roll(two, 64, 1)).astype(BF16)
        abuf[384:768, 128 * n : 128 * n + 128] = jnp.where(left, pltpu.roll(one, 64, 1), two).astype(BF16)
    local[4].wait()
    res.finish()
    for dx in (0, -1, 1, 2):
        share_res(dx).wait_send()

    def project(i, carry):
        for n in range(3):
            @pl.when(i == n)
            def _():
                w_event(8 + n)
        rows = pl.ds(pl.multiple_of(i * MT, MT), MT)
        wide = dot(abuf[rows, :], owbuf[...]) + mid[rows, :].astype(F32)
        middle = wide.astype(BF16)
        mid[rows, :] = middle
        wide = middle.astype(F32)
        scaled = wide * lax.rsqrt(jnp.mean(wide * wide, axis=-1, keepdims=True) + EPSILON)
        nbuf[rows, :] = (scaled * gain_ref[:, 256:].astype(F32)).astype(BF16)
        return carry

    lax.fori_loop(0, ROWS // MT, project, 0)
    w_event(11)

    def swap(n):
        return beside(xs.at[n], xr.at[n], d_s.at[n], d_r.at[n])

    def chunk(n, dx):
        rows = pl.ds(pl.multiple_of(at_x(dx) * 192, 64), 192)
        gate = dot(nbuf[rows, :], wbuf[0:FFD, :], 1, 1)
        upward = dot(nbuf[rows, :], wbuf[FFD : 2 * FFD, :], 1, 1)
        hidden = (gate / (1.0 + jnp.exp(-gate)) * upward).astype(BF16)
        part = dot(hidden, wbuf[2 * FFD : 3 * FFD, :]).astype(BF16)

        @pl.when(core == 0)
        def _():
            po[n] = part[0:96]
            xs[n] = part[96:192]

        @pl.when(core == 1)
        def _():
            po[n] = part[96:192]
            xs[n] = part[0:96]

        swap(n).start()

    def hop(src, dst, to, k):
        return pltpu.make_async_remote_copy(
            src_ref=src, dst_ref=dst, send_sem=f_s.at[k], recv_sem=f_r.at[k],
            device_id=to_x(to, 0), device_id_type=mesh_id,
        )

    def summed(n):
        swap(n).wait_recv()
        return po[n].astype(F32) + xr[n].astype(F32)

    chunk(0, 2)
    chunk(1, 1)
    st[0] = summed(0).astype(BF16)
    hops = [
        hop(st.at[0, pl.ds(0, 48)], ra, 1, 0),
        hop(st.at[0, pl.ds(48, 48)], rb, -1, 1),
        hop(st.at[1, pl.ds(48, 48)], fa.at[pl.ds(48, 48)], 1, 2),
        hop(st.at[2, pl.ds(0, 48)], fb.at[pl.ds(0, 48)], -1, 3),
        hop(so.at[0], fa.at[pl.ds(0, 48)], 1, 4),
        hop(so.at[1], fb.at[pl.ds(48, 48)], -1, 5),
    ]
    hops[0].start()
    hops[1].start()
    chunk(2, 3)
    ahead = summed(1)
    st[1, 48:96, :] = ahead[48:96].astype(BF16)
    hops[2].start()
    chunk(3, 0)
    behind = summed(2)
    st[2, 0:48, :] = behind[0:48].astype(BF16)
    hops[3].start()
    hops[0].wait_recv()
    so[0] = (po[1, 0:48, :].astype(F32) + xr[1, 0:48, :].astype(F32) + ra[...].astype(F32)).astype(BF16)
    hops[4].start()
    hops[1].wait_recv()
    so[1] = (behind[48:96] + rb[...].astype(F32)).astype(BF16)
    hops[5].start()
    total = summed(3) + mid[pl.ds(pl.multiple_of(tp * OWN, 32), OWN), :].astype(F32)
    for h in hops[2:]:
        h.wait_recv()
    out_ref[...] = (total + fa[...].astype(F32) + fb[...].astype(F32)).astype(BF16)

    for flow in (lat, w_a, w_b, att):
        flow.finish()
    for rel in others:
        for far in (0, 1):
            share_lat(rel, far).wait_send()
        for dx in (1, -1):
            cross(rel, dx).wait_send()
    for dx in (0, -1, 1, 2):
        share_att(dx).wait_send()
    for n in range(4):
        swap(n).wait_send()
    for h in hops:
        h.wait_send()


def on_device(
    resid, query_small, query_large, kv_latent, rope_key, kv_gain, up_key_small, up_value_small,
    up_key_large, up_value_large, out_weight, mix_gain, gate_weight, up_weight, down_weight,
):
    rows = kv_latent.shape[0]
    positions = lax.axis_index("sp") * rows + jnp.arange(rows, dtype=jnp.int32)
    inverse = THETA ** (-jnp.arange(0, ROTARY, 2).astype(F32) / ROTARY)
    phase = inverse[:, None] * positions.astype(F32)[None, :]
    trig = jnp.concatenate([jnp.cos(phase), jnp.sin(phase)], axis=0)
    gains = jnp.concatenate([kv_gain, mix_gain]).reshape(1, 256 + D)

    vmem = pl.BlockSpec(memory_space=pltpu.VMEM)
    hbm = pl.BlockSpec(memory_space=pl.ANY)
    dma = pltpu.SemaphoreType.DMA
    return pl.pallas_call(
        kernel,
        out_shape=jax.ShapeDtypeStruct((OWN, D), BF16),
        in_specs=[vmem] * 10 + [hbm] * 5,
        out_specs=vmem,
        scratch_shapes=[
            pltpu.VMEM((16, LAT_ROWS, 256), BF16),
            pltpu.VMEM((3 * FFD, D), BF16),
            pltpu.VMEM((1536, D), BF16),
            pltpu.VMEM((ROWS, D), BF16),
            pltpu.VMEM((ROWS, D), BF16),
            pltpu.VMEM((8, 1152, 128), BF16),
            pltpu.VMEM((ROWS, 1536), BF16),
            pltpu.VMEM((96, ROWS), BF16),
            pltpu.VMEM((160, ROWS), BF16),
            pltpu.VMEM((256, 192), BF16),
            pltpu.VMEM((192, 256), BF16),
            pltpu.VMEM((ROWS, 96), BF16),
            pltpu.VMEM((ROWS, 160), BF16),
            pltpu.VMEM((80, ROWS), BF16),
            pltpu.VMEM((144, ROWS), BF16),
            pltpu.VMEM((1, ROWS), F32),
            pltpu.VMEM((1, ROWS), F32),
            pltpu.VMEM((80, ROWS), F32),
            pltpu.VMEM((144, ROWS), F32),
            pltpu.VMEM((4, OWN, D), BF16),
            pltpu.VMEM((4, OWN, D), BF16),
            pltpu.VMEM((4, OWN, D), BF16),
            pltpu.VMEM((48, D), BF16),
            pltpu.VMEM((48, D), BF16),
            pltpu.VMEM((OWN, D), BF16),
            pltpu.VMEM((OWN, D), BF16),
            pltpu.VMEM((3, OWN, D), BF16),
            pltpu.VMEM((2, 48, D), BF16),
            dma((5,)),
            *[dma((20,)) for _ in range(6)],
            *[dma((2, 16)) for _ in range(4)],
            *[dma((4,)) for _ in range(8)],
            dma((4,)), dma((4,)), dma((6,)), dma((6,)),
        ],
        compiler_params=pltpu.CompilerParams(
            collective_id=0, has_side_effects=True, vmem_limit_bytes=67043328
        ),
    )(
        kv_latent, rope_key.T, trig, gains, query_small.T, query_large.T,
        up_key_small.T, up_key_large, up_value_small.T, up_value_large,
        out_weight, resid, gate_weight.T, up_weight.T, down_weight.T,
    )


def solution(mesh):
    placed = (
        P(("sp", "tp"), None), P("sp", "tp"), P("sp", "tp"), P("sp", None), P("sp", None), P(),
        P(None, "tp"), P(None, "tp"), P(None, "tp"), P(None, "tp"), P(), P(),
        P("sp", "tp"), P("sp", "tp"), P("sp", "tp"),
    )
    return jax.shard_map(
        on_device, mesh=mesh, in_specs=placed, out_specs=P(("sp", "tp"), None), check_vma=False
    )
```
